128 devices in a mesh: sp: 16 (over z, y), tp: 8 (over x, core).
Axes of the slice: x: 4, y: 4, z: 4, core: 2. Of those that a mesh axis runs over, the one named last changes fastest.
Arguments:
- arriving_hidden_state: bfloat16 [16384, 2048], P(('sp', 'tp')), may hold values from -6 to 6
- former_request_vectors: bfloat16 [16384, 1024], P('sp', 'tp'), may hold values from -6 to 6
- former_match_vectors: bfloat16 [16384, 1024], P('sp', 'tp'), may hold values from -6 to 6
- latter_request_vectors: bfloat16 [16384, 512], P('sp', 'tp'), may hold values from -6 to 6
- latter_match_vectors: bfloat16 [16384, 512], P('sp', 'tp'), may hold values from -6 to 6
- stored_vectors_both: bfloat16 [16384, 2, 1024], P('sp', None, 'tp'), may hold values from -6 to 6
- closing_valve_operands: bfloat16 [16384, 2, 1024], P('sp', None, 'tp'), may hold values from -6 to 6
- update_level_before_squash: bfloat16 [2, 8, 16384], P(None, 'tp', 'sp'), may hold values from -4 to -3
- fading_data_input: float32 [2, 8, 16384], P(None, 'tp', 'sp'), may hold values from -5.5 to 5.5
- sparse_fading_boost: float32 [2, 8, 16384], P(None, 'tp', 'sp'), may hold values from -2 to 0, as said below
- unitwise_fading_loglevel: float32 [2, 8], P(None, 'tp'), as said below
- fading_constant_term: float32 [2, 8], P(None, 'tp'), may hold values from -1 to 1
- unitwise_normalizer_coef: float32 [128], replicated, may hold values from 0.1 to 1.9
- emission_map_weights: bfloat16 [2048, 2048], replicated, may hold values from -0.125 to 0.125
- channel_normalizer_coef: float32 [2048], replicated, may hold values from 0.1 to 1.9
- switching_channel_map: bfloat16 [2048, 6144], P('sp', 'tp'), may hold values from -0.125 to 0.125
- broadening_channel_map: bfloat16 [2048, 6144], P('sp', 'tp'), may hold values from -0.125 to 0.125
- timewise_convolve_tapvalues: bfloat16 [3, 2, 6144], P(None, None, 'tp'), may hold values from -3.5 to 3.5
- narrowing_map_weights_in: bfloat16 [2048, 6144], P('sp', 'tp'), may hold values from -0.078125 to 0.078125
Outputs:
- mixed: bfloat16 [16384, 2048], P(('sp', 'tp'))
The draws below stay inside these ranges and needn't reach their ends.
Inputs may be any that keep to these rules, and one draw needn't show every extreme that they name: `unitwise_fading_loglevel`: each entry is the logarithm of a per-position rate between 0.2 / 16384 and 2 / 64. `sparse_fading_boost`: zero except at three or fewer positions of the sequence.
All inputs are finite; a program needn't handle non-finite values.
Results may differ from the reference program's by a relative error of at most 0.015.
Values may be sent and summed in bfloat16 or wider, within the bound.
A program may use at most 128 MiB of HBM per device.

```python
import jax
import jax.numpy as jnp
from jax import lax

MODEL_WIDTH = 2048
ATTN_UNITS = 8
DK_ONE = 128
DK_TWO = 64
VALUE_DIM = 128
FF = 6144
SPAN = 64
TAPS = 3
TOK_DEV = 1024
STEP_TOTAL = 16384
VW = 2048
N_TP = 8


def drawn_keys(key, column_count):
    direction_key, jitter_key = jax.random.split(key)
    directions = jax.random.normal(direction_key, (STEP_TOTAL // SPAN, column_count), jnp.float32)
    repeated = jnp.repeat(directions, SPAN, axis=0)
    jitter = jax.random.normal(jitter_key, (STEP_TOTAL, column_count), jnp.float32)
    jitter_scale = 0.2
    return jnp.clip(repeated + jitter_scale * jitter, -6.0, 6.0).astype(jnp.bfloat16)


def draw_former_match_vectors(key, part):
    return drawn_keys(jax.random.fold_in(key, 71), ATTN_UNITS * DK_ONE)


def draw_latter_match_vectors(key, part):
    return drawn_keys(jax.random.fold_in(key, 79), ATTN_UNITS * DK_TWO)


def draw_update_level_before_squash(key, part):
    drawn = jax.random.uniform(jax.random.fold_in(key, 53), (2, ATTN_UNITS, STEP_TOTAL), jnp.float32, -4.0, -3.0)
    return drawn.astype(jnp.bfloat16)


def draw_fading_data_input(key, part):
    noise_key, shift_key = jax.random.split(jax.random.fold_in(key, 11))
    noise_draw = jax.random.truncated_normal(noise_key, -4.0, 4.0, (2, ATTN_UNITS, STEP_TOTAL), jnp.float32)
    offsets = jax.random.uniform(shift_key, (2, ATTN_UNITS, STEP_TOTAL // TOK_DEV), jnp.float32, -1.5, 1.5)
    offset_rows = jnp.repeat(offsets, TOK_DEV, axis=2)
    return noise_draw + offset_rows


def draw_sparse_fading_boost(key, part):
    position_random_key, size_key = jax.random.split(jax.random.fold_in(key, 23))
    spike_positions = jax.random.randint(position_random_key, (3,), 0, STEP_TOTAL)
    kept_share = jax.random.uniform(size_key, (2, ATTN_UNITS, 3), jnp.float32, 0.55, 0.8)
    position_hits = (jnp.arange(STEP_TOTAL)[None, :] == spike_positions[:, None]).astype(jnp.float32)
    return jnp.einsum('ghb,bs->ghs', jnp.log(kept_share), position_hits)


def draw_unitwise_fading_loglevel(key, part):
    pick_key, fast_key, slow_key = jax.random.split(jax.random.fold_in(key, 37), 3)
    fast_share = 0.5
    fast_mask = jax.random.uniform(pick_key, (2, ATTN_UNITS), jnp.float32) < fast_share
    fast_rate = jax.random.uniform(fast_key, (2, ATTN_UNITS), jnp.float32, 1.0, 2.0) / SPAN
    slow_rate = jax.random.uniform(slow_key, (2, ATTN_UNITS), jnp.float32, 0.2, 0.4) / STEP_TOTAL
    return jnp.log(jnp.where(fast_mask, fast_rate, slow_rate))


def level_of(key, dims, cuts, smallest, high):
    loudness, own = 1.0, jax.random.fold_in(key, 6)
    for axis_at, shards_of in cuts:
        heights = jnp.exp(jax.random.uniform(jax.random.fold_in(own, axis_at), (shards_of,), jnp.float32, smallest / len(cuts), high / len(cuts)))
        loudness = loudness * jnp.repeat(heights, dims[axis_at] // shards_of).reshape([-1 if axis == axis_at else 1 for axis in range(len(dims))])
    return loudness


def gaussian(rng, shape, scale, most, shards=(), kind=jnp.bfloat16):
    entries = jax.random.normal(rng, shape, jnp.float32) * scale
    if len(shards) > 0:
        entries = level_of(rng, shape, shards, -0.22, 0.18) * entries
    return jnp.clip(entries, min=-most, max=most).astype(kind)


def setup_inputs(seed: int = 0) -> dict:
    streams_of = jax.random.split(jax.random.key(seed), 20)
    return {
        "arriving_hidden_state": gaussian(streams_of[0], (STEP_TOTAL, MODEL_WIDTH), 1.0, 6.0, ((0, 128),)),
        "former_request_vectors": gaussian(streams_of[1], (STEP_TOTAL, ATTN_UNITS * DK_ONE), 1.0, 6.0, ((0, 16), (1, 8))),
        "former_match_vectors": draw_former_match_vectors(jax.random.fold_in(streams_of[19], 71), 0),
        "latter_request_vectors": gaussian(streams_of[3], (STEP_TOTAL, ATTN_UNITS * DK_TWO), 1.0, 6.0, ((0, 16), (1, 8))),
        "latter_match_vectors": draw_latter_match_vectors(jax.random.fold_in(streams_of[19], 71), 0),
        "stored_vectors_both": gaussian(streams_of[5], (STEP_TOTAL, 2, ATTN_UNITS * VALUE_DIM), 1.0, 6.0, ((0, 16), (2, 8))),
        "closing_valve_operands": gaussian(streams_of[6], (STEP_TOTAL, 2, ATTN_UNITS * VALUE_DIM), 1.0, 6.0, ((0, 16), (2, 8))),
        "update_level_before_squash": draw_update_level_before_squash(jax.random.fold_in(streams_of[19], 71), 0),
        "fading_data_input": draw_fading_data_input(jax.random.fold_in(streams_of[19], 71), 0),
        "sparse_fading_boost": draw_sparse_fading_boost(jax.random.fold_in(streams_of[19], 71), 0),
        "unitwise_fading_loglevel": draw_unitwise_fading_loglevel(jax.random.fold_in(streams_of[19], 71), 0),
        "fading_constant_term": jnp.clip(jax.random.uniform(streams_of[11], (2, ATTN_UNITS), jnp.float32, -1.0, 1.0) * level_of(streams_of[11], (2, ATTN_UNITS), ((1, 8),), -0.4, 0.0), -1.0, 1.0),
        "unitwise_normalizer_coef": jnp.clip(1.0 + 0.18 * jax.random.normal(streams_of[12], (VALUE_DIM,), jnp.float32), 0.1, 1.9),
        "emission_map_weights": gaussian(streams_of[13], (VW, MODEL_WIDTH), VW ** -0.5, 0.125),
        "channel_normalizer_coef": jnp.clip(1.0 + 0.18 * jax.random.normal(streams_of[14], (MODEL_WIDTH,), jnp.float32), 0.1, 1.9),
        "switching_channel_map": gaussian(streams_of[15], (MODEL_WIDTH, FF), MODEL_WIDTH ** -0.5, 0.125, ((0, 16), (1, 8))),
        "broadening_channel_map": gaussian(streams_of[16], (MODEL_WIDTH, FF), MODEL_WIDTH ** -0.5, 0.125, ((0, 16), (1, 8))),
        "timewise_convolve_tapvalues": gaussian(streams_of[17], (TAPS, 2, FF), TAPS ** -0.5, 3.5, ((2, 8),)),
        "narrowing_map_weights_in": gaussian(streams_of[18], (MODEL_WIDTH, FF), FF ** -0.5, 0.078125, ((0, 16), (1, 8))),
    }


EPSILON = 1e-06
PRECISE = lax.Precision.HIGHEST

def unit_rows(matrix):
    return matrix * lax.rsqrt(lax.optimization_barrier(jnp.sum(matrix * matrix, axis=-1, keepdims=True)) + EPSILON)

def heads_first(matrix, head_count):
    row_count = matrix.shape[0]
    return matrix.reshape(row_count, head_count, -1).astype(jnp.float32).transpose(1, 0, 2)

def block_terms(queries, key_rows, value_rows, beta_rate, gate_logarithms):
    head_count, length, key_size = queries.shape
    num_blocks = length // SPAN
    queries = queries.reshape(head_count, num_blocks, SPAN, -1)
    key_rows = key_rows.reshape(head_count, num_blocks, SPAN, -1)
    value_rows = value_rows.reshape(head_count, num_blocks, SPAN, -1)
    beta_rate = beta_rate.reshape(head_count, num_blocks, SPAN)
    cum_gates = jnp.cumsum(gate_logarithms.reshape(head_count, num_blocks, SPAN), axis=-1)
    row_pos = lax.broadcasted_iota(jnp.int32, (SPAN, SPAN), 0)
    col_pos = lax.broadcasted_iota(jnp.int32, (SPAN, SPAN), 1)
    causal = row_pos >= col_pos
    strict = row_pos > col_pos
    decay = jnp.exp(jnp.where(causal, cum_gates[..., :, None] - cum_gates[..., None, :], -jnp.inf))
    key_beta = key_rows * beta_rate[..., None]
    lower = jnp.where(strict, jnp.einsum('hncd,hnsd->hncs', key_beta, key_rows, precision=PRECISE) * decay, 0.0)
    right_side = jnp.concatenate([value_rows * beta_rate[..., None], key_beta * jnp.exp(cum_gates)[..., None]], axis=-1)
    unit_mat = jnp.eye(SPAN, dtype=lower.dtype)
    solved = lax.linalg.triangular_solve(lower + unit_mat, right_side, left_side=True, lower=True, unit_diagonal=True)
    value_size = value_rows.shape[-1]
    u_values = solved[..., :value_size]
    w_keys = solved[..., value_size:]
    intra = jnp.einsum('hncd,hnsd->hncs', queries, key_rows, precision=PRECISE) * decay
    key_decayed = key_rows * jnp.exp(cum_gates[..., -1:] - cum_gates)[..., None]
    return (queries, u_values, w_keys, intra, key_decayed, cum_gates)

def run_blocks(increment_list, initial_memory):

    def advance(state_mat, inputs):
        query_blk, u_blk, w_blk, intra_blk, kdec_blk, cum_blk = inputs
        fresh = u_blk - jnp.einsum('hcd,hde->hce', w_blk, state_mat, precision=PRECISE)
        output = jnp.einsum('hcd,hde->hce', query_blk * jnp.exp(cum_blk)[..., None], state_mat, precision=PRECISE)
        output = output + jnp.einsum('hcs,hse->hce', intra_blk, fresh, precision=PRECISE)
        state_mat = state_mat * jnp.exp(cum_blk[:, -1])[:, None, None]
        state_mat = state_mat + jnp.einsum('hcd,hce->hde', kdec_blk, fresh, precision=PRECISE)
        return (state_mat, output)
    moved = tuple((jnp.moveaxis(member, 1, 0) for member in increment_list))
    _, outputs = lax.scan(advance, initial_memory, moved)
    head_count = outputs.shape[1]
    return jnp.moveaxis(outputs, 0, 1).reshape(head_count, -1, outputs.shape[-1])

def team_parts(asker_weights, lookup_weights, value_matrix, correction_draw, decay_draw, spike_draw, decay_logarithm, bias_vector):
    head_count = decay_logarithm.shape[0]
    queries = heads_first(asker_weights, head_count)
    key_size = queries.shape[-1]
    queries = unit_rows(queries) * key_size ** (-0.5)
    key_rows = unit_rows(heads_first(lookup_weights, head_count))
    value_rows = heads_first(value_matrix, head_count)
    beta_rate = jax.nn.sigmoid(correction_draw.astype(jnp.float32))
    gate_logarithms = -jnp.exp(decay_logarithm)[:, None] * jax.nn.softplus(decay_draw + bias_vector[:, None]) + spike_draw
    return block_terms(queries, key_rows, value_rows, beta_rate, gate_logarithms)

def completed_attn_units(increment_list, initial_memory, gate_cols, unitwise_normalizer_coef):
    outputs = run_blocks(increment_list, initial_memory)
    head_count = outputs.shape[0]
    gates_in = heads_first(gate_cols, head_count)
    scaled = outputs * lax.rsqrt(lax.optimization_barrier(jnp.mean(outputs * outputs, axis=-1, keepdims=True)) + EPSILON) * unitwise_normalizer_coef
    scaled = scaled * jax.nn.silu(gates_in)
    return scaled.transpose(1, 0, 2).reshape(outputs.shape[1], -1).astype(jnp.bfloat16)

def causal_taps(low_rows, taps_col):
    padded = jnp.concatenate([jnp.zeros((TAPS - 1, low_rows.shape[1]), low_rows.dtype), low_rows], axis=0)
    length = low_rows.shape[0]
    total = taps_col[0] * padded[0:length]
    for tap_index in range(1, TAPS):
        total = total + taps_col[tap_index] * padded[tap_index:tap_index + length]
    return total

def reference(arriving_hidden_state, former_request_vectors, former_match_vectors, latter_request_vectors, latter_match_vectors, stored_vectors_both, closing_valve_operands, update_level_before_squash, fading_data_input, sparse_fading_boost, unitwise_fading_loglevel, fading_constant_term, unitwise_normalizer_coef, emission_map_weights, channel_normalizer_coef, switching_channel_map, broadening_channel_map, timewise_convolve_tapvalues, narrowing_map_weights_in):
    combined_attn_units = []
    pairs = ((former_request_vectors, former_match_vectors), (latter_request_vectors, latter_match_vectors))
    for cohort_ordinal in range(2):
        asker_weights, lookup_weights = pairs[cohort_ordinal]
        increment_list = team_parts(asker_weights, lookup_weights, stored_vectors_both[:, cohort_ordinal], update_level_before_squash[cohort_ordinal], fading_data_input[cohort_ordinal], sparse_fading_boost[cohort_ordinal], unitwise_fading_loglevel[cohort_ordinal], fading_constant_term[cohort_ordinal])
        key_size = increment_list[0].shape[-1]
        head_count = unitwise_fading_loglevel.shape[1]
        initial_memory = jnp.zeros((head_count, key_size, stored_vectors_both.shape[-1] // head_count), jnp.float32)
        combined_attn_units.append(completed_attn_units(increment_list, initial_memory, closing_valve_operands[:, cohort_ordinal], unitwise_normalizer_coef))
    linear_attend = jnp.stack(combined_attn_units, axis=1)
    token_slices = linear_attend.shape[0]
    skip_stream = arriving_hidden_state.astype(jnp.float32) + jnp.dot(linear_attend.reshape(token_slices, -1).astype(jnp.float32), emission_map_weights.astype(jnp.float32), preferred_element_type=jnp.float32)
    normed = (skip_stream * lax.rsqrt(lax.optimization_barrier(jnp.mean(skip_stream * skip_stream, axis=-1, keepdims=True)) + EPSILON) * channel_normalizer_coef).astype(jnp.bfloat16)
    gate_low = jnp.dot(normed.astype(jnp.float32), switching_channel_map.astype(jnp.float32), preferred_element_type=jnp.float32).astype(jnp.bfloat16)
    up_low = jnp.dot(normed.astype(jnp.float32), broadening_channel_map.astype(jnp.float32), preferred_element_type=jnp.float32).astype(jnp.bfloat16)
    taps = timewise_convolve_tapvalues.astype(jnp.float32)
    gate_conv = causal_taps(gate_low, taps[:, 0])
    up_conv = causal_taps(up_low, taps[:, 1])
    hidden = (jax.nn.silu(gate_conv) * up_conv).astype(jnp.bfloat16)
    shard_width = hidden.shape[1] // N_TP
    down_sum = jnp.zeros(skip_stream.shape, jnp.float32)
    for shard_index in range(N_TP):
        lower_col = shard_index * shard_width
        partial_value = lax.dot_general(hidden[:, lower_col:lower_col + shard_width].astype(jnp.float32), narrowing_map_weights_in[:, lower_col:lower_col + shard_width].astype(jnp.float32), (((1,), (1,)), ((), ())), preferred_element_type=jnp.float32)
        down_sum = down_sum + lax.optimization_barrier(partial_value.astype(jnp.bfloat16)).astype(jnp.float32)
    return (skip_stream + down_sum).astype(jnp.bfloat16)
```

```python
import jax
import jax.numpy as jnp
from jax import lax
from jax.experimental import pallas as pl
from jax.experimental.pallas import tpu as pltpu
from jax.sharding import Mesh
from jax.sharding import PartitionSpec as P

TAPS = 3
SP = ("sp_0", "sp_1")
SP_TP = ("sp_0", "sp_1", "tp")

BLK = 128
NBLK = 8
EPSILON = 1e-06
F32 = jnp.float32
BF16 = jnp.bfloat16


def mm(a, b):
    return jnp.dot(a.astype(BF16), b.astype(BF16), preferred_element_type=F32)


def mm_nt(a, b):
    return lax.dot_general(
        a.astype(BF16), b.astype(BF16), (((1,), (1,)), ((), ())), preferred_element_type=F32
    )


def normed_rows(x, scale):
    return x * (lax.rsqrt(jnp.sum(x * x, axis=-1, keepdims=True) + EPSILON) * scale)


def fold_blocks(row):
    return jnp.concatenate([row[:, i * BLK : (i + 1) * BLK] for i in range(NBLK)], axis=0)


def gate_rows(upd, fade, boost, loglevel, bias):
    beta = 1.0 / (1.0 + jnp.exp(-fold_blocks(upd.astype(F32))))
    pre = fold_blocks(fade) + bias
    soft = jnp.maximum(pre, 0.0) + jnp.log1p(jnp.exp(-jnp.abs(pre)))
    rate = jnp.exp(jnp.full((NBLK, BLK), loglevel, F32))
    cum = fold_blocks(boost) - rate * soft
    lane = lax.broadcasted_iota(jnp.int32, (NBLK, BLK), 1)
    step = 1
    while step < BLK:
        cum = cum + jnp.where(lane >= step, pltpu.roll(cum, step, 1), 0.0)
        step *= 2
    return beta, cum


def block_inputs(q, k, v, cum_row, beta_row):
    dk = q.shape[-1]
    c_j = jnp.broadcast_to(cum_row, (BLK, BLK))
    c_i = c_j.T
    b_i = jnp.broadcast_to(beta_row, (BLK, BLK)).T
    row = lax.broadcasted_iota(jnp.int32, (BLK, BLK), 0)
    col = lax.broadcasted_iota(jnp.int32, (BLK, BLK), 1)
    decay = jnp.exp(jnp.where(row >= col, c_i - c_j, -1e30))
    e_i = jnp.exp(c_i)
    c_last = jnp.broadcast_to(cum_row[:, BLK - 1 :], (1, BLK))
    qn = normed_rows(q.astype(F32), dk**-0.5)
    kn = normed_rows(k.astype(F32), 1.0)
    kb = kn.astype(BF16)
    both = mm_nt(jnp.concatenate([kb, qn.astype(BF16)], axis=0), kb)
    lower = jnp.where(row > col, -(b_i * both[:BLK] * decay), 0.0)
    intra = (both[BLK:] * decay).astype(BF16)
    right = jnp.concatenate([v.astype(F32) * b_i, kn * (b_i * e_i)[:, :dk]], axis=1)
    tail = kn * jnp.exp(c_last - c_i)[:, :dk]
    return dict(
        lower=lower,
        intra=intra,
        right=right,
        tail=tail.T.astype(BF16),
        query=qn * e_i[:, :dk],
        keep=jnp.exp(c_last),
    )


def inverses(lowers):
    powers = [n.astype(BF16) for n in lowers]
    extra = list(lowers)
    power = [mm(p, p) for p in powers]
    for level in range(1, 7):
        pb = [p.astype(BF16) for p in power]
        if level < 6:
            wide = [
                mm(p, jnp.concatenate([e.astype(BF16), p], axis=1)) for p, e in zip(pb, extra)
            ]
            extra = [e + p + w[:, :BLK] for e, p, w in zip(extra, power, wide)]
            power = [w[:, BLK:] for w in wide]
        else:
            extra = [e + p + mm(q, e) for e, p, q in zip(extra, power, pb)]
    return extra


def local_kernel(
    q1, k1, q2, k2, vals, upd, fade, boost, level, bias,
    r1, r2, o1, o2, pay,
    beta_s, cum_s, keep_s, qd1, qd2, loc1, loc2, add1, add2,
):
    for h in range(2):
        beta, cum = gate_rows(upd[h], fade[h], boost[h], level[h, 0], bias[h, 0])
        beta_s[h * NBLK : (h + 1) * NBLK, :] = beta
        cum_s[h * NBLK : (h + 1) * NBLK, :] = cum

    def parts(it, carry):
        todo = [(h, 2 * it + j) for j in range(2) for h in range(2)]
        ins = []
        for h, n in todo:
            rows = pl.ds(pl.multiple_of(n * BLK, BLK), BLK)
            q, k = (q1, k1) if h == 0 else (q2, k2)
            ins.append(
                block_inputs(
                    q[rows, :],
                    k[rows, :],
                    vals[rows, h * BLK : (h + 1) * BLK],
                    cum_s[pl.ds(h * NBLK + n, 1), :],
                    beta_s[pl.ds(h * NBLK + n, 1), :],
                )
            )
        extra = inverses([i["lower"] for i in ins])
        for (h, n), i, e in zip(todo, ins, extra):
            dk = (128, 64)[h]
            solved = (i["right"] + mm(e, i["right"])).astype(BF16)
            made = mm(jnp.concatenate([i["intra"], i["tail"]], axis=0), solved)
            qd, loc, add = ((qd1, loc1, add1), (qd2, loc2, add2))[h]
            qd[n, :BLK, :] = (i["query"] - made[:BLK, BLK:]).astype(BF16)
            qd[n, BLK:, :] = (-made[BLK:, BLK:]).astype(BF16)
            loc[n] = made[:BLK, :BLK]
            add[n] = made[BLK:, :BLK]
            keep_s[pl.ds(h * NBLK + n, 1), :] = i["keep"]
        return carry

    lax.fori_loop(0, NBLK // 2, parts, 0)

    def eye(dk):
        return (
            lax.broadcasted_iota(jnp.int32, (dk, dk), 0)
            == lax.broadcasted_iota(jnp.int32, (dk, dk), 1)
        ).astype(F32)

    def chain(n, carry):
        rows = pl.ds(pl.multiple_of(n * BLK, BLK), BLK)
        out = []
        for h, (state, total) in enumerate(carry):
            dk = (128, 64)[h]
            qd, loc, add = ((qd1, loc1, add1), (qd2, loc2, add2))[h]
            r, o = ((r1, o1), (r2, o2))[h]
            made = mm(qd[n], state)
            o[rows, :] = loc[n] + made[:BLK, :BLK]
            r[rows, :] = made[:BLK, BLK:].astype(BF16)
            keep = keep_s[pl.ds(h * NBLK + n, 1), :]
            moved = made[BLK:]
            new_a = state[:, :BLK] * keep + moved[:, :BLK] + add[n]
            new_p = state[:, BLK:] * keep[:, :dk] + moved[:, BLK:]
            out.append((jnp.concatenate([new_a, new_p], axis=1), total * keep))
        return tuple(out)

    start = tuple(
        (jnp.concatenate([jnp.zeros((dk, BLK), F32), eye(dk)], axis=1), jnp.ones((1, BLK), F32))
        for dk in (128, 64)
    )
    (s1, g1), (s2, g2) = lax.fori_loop(0, NBLK, chain, start)
    pay[0:128, :] = (s1[:, BLK:] - eye(128) * g1).astype(BF16)
    pay[128:256, :] = s1[:, :BLK].astype(BF16)
    pay[256:320, :] = s2[:, :BLK].astype(BF16)
    row = lax.broadcasted_iota(jnp.int32, (64, 64), 0)
    hi1, hi2 = g1.astype(BF16).astype(F32), g2.astype(BF16).astype(F32)
    scal = jnp.where(row == 0, hi1[:, :64], 0.0)
    scal = scal + jnp.where(row == 1, (g1 - hi1)[:, :64], 0.0)
    scal = scal + jnp.where(row == 2, hi2[:, :64], 0.0)
    scal = scal + jnp.where(row == 3, (g2 - hi2)[:, :64], 0.0)
    d2 = s2[:, BLK:] - eye(64) * g2[:, :64]
    pay[320:384, :] = jnp.concatenate([d2, scal], axis=1).astype(BF16)


def local_recurrence(q1, k1, q2, k2, vals, upd, fade, boost, level, bias):
    vm = pl.BlockSpec(memory_space=pltpu.VMEM)
    sm = pl.BlockSpec(memory_space=pltpu.SMEM)
    return pl.pallas_call(
        local_kernel,
        out_shape=(
            jax.ShapeDtypeStruct((1024, 128), BF16),
            jax.ShapeDtypeStruct((1024, 64), BF16),
            jax.ShapeDtypeStruct((1024, 128), F32),
            jax.ShapeDtypeStruct((1024, 128), F32),
            jax.ShapeDtypeStruct((384, 128), BF16),
        ),
        in_specs=[vm] * 8 + [sm] * 2,
        out_specs=[vm] * 5,
        scratch_shapes=[
            pltpu.VMEM((2 * NBLK, BLK), F32),
            pltpu.VMEM((2 * NBLK, BLK), F32),
            pltpu.VMEM((2 * NBLK, BLK), F32),
            pltpu.VMEM((NBLK, 256, 128), BF16),
            pltpu.VMEM((NBLK, 192, 64), BF16),
            pltpu.VMEM((NBLK, BLK, BLK), F32),
            pltpu.VMEM((NBLK, BLK, BLK), F32),
            pltpu.VMEM((NBLK, 128, BLK), F32),
            pltpu.VMEM((NBLK, 64, BLK), F32),
        ],
        cost_estimate=pl.CostEstimate(
            flops=2_000_000_000, bytes_accessed=4_000_000, transcendentals=1_000_000
        ),
    )(q1, k1, q2, k2, vals, upd, fade, boost, level, bias)


def split_pay(pay):
    p = pay.astype(F32)
    g1 = p[320, 64] + p[321, 64]
    g2 = p[322, 64] + p[323, 64]
    return (p[:128], p[128:256], g1), (p[320:, :64], p[256:320], g2)


def join_pay(one, two):
    (d1, a1, g1), (d2, a2, g2) = one, two
    hi1, hi2 = lax.reduce_precision(g1, 8, 7), lax.reduce_precision(g2, 8, 7)
    scal = jnp.stack([hi1, g1 - hi1, hi2, g2 - hi2])
    scal = jnp.pad(jnp.broadcast_to(scal[:, None], (4, 64)), ((0, 60), (0, 0)))
    low = jnp.concatenate([d2, scal], axis=1)
    return jnp.concatenate([d1, a1, a2, low], axis=0).astype(BF16)


def after(earlier, later):
    d0, a0, g0 = earlier
    d1, a1, g1 = later
    return (g1 * d0 + g0 * d1 + mm(d1, d0), g1 * a0 + a1 + mm(d1, a0), g0 * g1)


def applied(later, state):
    d, a, g = later
    return g * state + a + mm(d, state)


def incoming_states(pay):
    y, z = lax.axis_index("sp_1"), lax.axis_index("sp_0")
    row = lax.all_gather(pay, "sp_1")
    members = [split_pay(row[i]) for i in range(4)]
    whole = members[0]
    for m in members[1:]:
        whole = tuple(after(e, l) for e, l in zip(whole, m))
    rows = lax.all_gather(join_pay(*whole), "sp_0")
    states = [jnp.zeros((128, 128), F32), jnp.zeros((64, 128), F32)]
    for i in range(3):
        states = [
            jnp.where(i < z, applied(m, s), s) for m, s in zip(split_pay(rows[i]), states)
        ]
    for i in range(3):
        states = [jnp.where(i < y, applied(m, s), s) for m, s in zip(members[i], states)]
    return states


def finished_head(local, reads, state, gate_cols, coef):
    out = local + mm(reads, state)
    scaled = out * lax.rsqrt(jnp.mean(out * out, axis=-1, keepdims=True) + EPSILON) * coef
    return (scaled * jax.nn.silu(gate_cols.astype(F32))).astype(BF16)


def from_behind(value, axis, steps):
    count = lax.axis_size(axis)
    leading, last = (max(0, -steps), min(count, count - steps))
    return lax.ppermute(value, axis, [(source, source + steps) for source in range(leading, last)])


def split_up(shard, dim, size):
    lengths = shard.shape
    tiles = shard.reshape(*lengths[:dim], size, lengths[dim] // size, *lengths[dim + 1 :])
    return jnp.moveaxis(tiles, dim, 0)


def summed_on_arrival(shard, axis, dim):
    tiles = split_up(shard, dim, lax.axis_size(axis))
    arrived = lax.all_to_all(tiles, axis, split_axis=0, concat_axis=0, tiled=True)
    return arrived.astype(jnp.float32).sum(axis=0)


def causal_taps(edge_rows, low_rows, taps_col):
    padded = jnp.concatenate([edge_rows, low_rows], axis=0)
    length = low_rows.shape[0]
    total = taps_col[0] * padded[0:length]
    for tap_index in range(1, TAPS):
        total = total + taps_col[tap_index] * padded[tap_index : tap_index + length]
    return total


def per_device(
    arriving_hidden_state,
    former_request_vectors,
    former_match_vectors,
    latter_request_vectors,
    latter_match_vectors,
    stored_vectors_both,
    closing_valve_operands,
    update_level_before_squash,
    fading_data_input,
    sparse_fading_boost,
    unitwise_fading_loglevel,
    fading_constant_term,
    unitwise_normalizer_coef,
    emission_map_weights,
    channel_normalizer_coef,
    switching_channel_map,
    broadening_channel_map,
    timewise_convolve_tapvalues,
    narrowing_map_weights_in,
):
    gathered = lax.all_gather(
        jnp.concatenate(
            [switching_channel_map, broadening_channel_map, narrowing_map_weights_in], axis=1
        ),
        SP,
        axis=0,
        tiled=True,
    )
    vals = stored_vectors_both.reshape(-1, 256)
    r1, r2, o1, o2, pay = local_recurrence(
        former_request_vectors,
        former_match_vectors,
        latter_request_vectors,
        latter_match_vectors,
        vals,
        update_level_before_squash,
        fading_data_input,
        sparse_fading_boost,
        unitwise_fading_loglevel,
        fading_constant_term,
    )
    s1, s2 = incoming_states(pay)
    linear_attend = jnp.stack(
        [
            finished_head(o1, r1, s1, closing_valve_operands[:, 0], unitwise_normalizer_coef),
            finished_head(o2, r2, s2, closing_valve_operands[:, 1], unitwise_normalizer_coef),
        ],
        axis=1,
    )
    arrived = lax.all_to_all(linear_attend, "tp", split_axis=0, concat_axis=2, tiled=True)
    row_count = arrived.shape[0]
    skip_stream = arriving_hidden_state.astype(jnp.float32) + jnp.dot(
        arrived.reshape(row_count, -1), emission_map_weights, preferred_element_type=jnp.float32
    )
    normed = (
        skip_stream
        * lax.rsqrt(jnp.mean(skip_stream * skip_stream, axis=-1, keepdims=True) + EPSILON)
        * channel_normalizer_coef
    ).astype(jnp.bfloat16)
    features = lax.all_gather(normed, "tp", axis=0, tiled=True)
    gate_full = jnp.dot(features, gathered[:, :768], preferred_element_type=jnp.float32)
    up_full = jnp.dot(features, gathered[:, 768:1536], preferred_element_type=jnp.float32)
    gate_low = gate_full.astype(jnp.bfloat16)
    up_low = up_full.astype(jnp.bfloat16)
    edge_gate, edge_up = from_behind((gate_low[-(TAPS - 1) :], up_low[-(TAPS - 1) :]), SP, 1)
    taps = timewise_convolve_tapvalues.astype(jnp.float32)
    gate_conv = causal_taps(edge_gate, gate_low, taps[:, 0])
    up_conv = causal_taps(edge_up, up_low, taps[:, 1])
    hidden = (jax.nn.silu(gate_conv) * up_conv).astype(jnp.bfloat16)
    down_sum = summed_on_arrival(
        lax.dot_general(
            hidden, gathered[:, 1536:], (((1,), (1,)), ((), ())), preferred_element_type=jnp.float32
        ).astype(jnp.bfloat16),
        "tp",
        0,
    )
    return (skip_stream + down_sum).astype(jnp.bfloat16)


def solution(mesh):
    torus = Mesh(mesh.devices.reshape(4, 4, mesh.shape["tp"]), ("sp_0", "sp_1", "tp"))
    return jax.shard_map(
        per_device,
        mesh=torus,
        in_specs=(
            P(SP_TP, None),
            P(SP, "tp"),
            P(SP, "tp"),
            P(SP, "tp"),
            P(SP, "tp"),
            P(SP, None, "tp"),
            P(SP, None, "tp"),
            P(None, "tp", SP),
            P(None, "tp", SP),
            P(None, "tp", SP),
            P(None, "tp"),
            P(None, "tp"),
            P(),
            P(),
            P(),
            P(SP, "tp"),
            P(SP, "tp"),
            P(None, None, "tp"),
            P(SP, "tp"),
        ),
        out_specs=P(SP_TP, None),
        check_vma=False,
    )
```

```python
import jax
import jax.numpy as jnp
from jax import lax
from jax.experimental import pallas as pl
from jax.experimental.pallas import tpu as pltpu
from jax.sharding import Mesh
from jax.sharding import PartitionSpec as P

TAPS = 3
SP = ("sp_0", "sp_1")
SP_TP = ("sp_0", "sp_1", "tp")

BLK = 128
NBLK = 8
EPSILON = 1e-06
F32 = jnp.float32
BF16 = jnp.bfloat16


def mm(a, b):
    return jnp.dot(a.astype(BF16), b.astype(BF16), preferred_element_type=F32)


def mm_nt(a, b):
    return lax.dot_general(
        a.astype(BF16), b.astype(BF16), (((1,), (1,)), ((), ())), preferred_element_type=F32
    )


def normed_rows(x, scale):
    return x * (lax.rsqrt(jnp.sum(x * x, axis=-1, keepdims=True) + EPSILON) * scale)


def fold_blocks(row):
    return jnp.concatenate([row[:, i * BLK : (i + 1) * BLK] for i in range(NBLK)], axis=0)


def gate_rows(upd, fade, boost, loglevel, bias):
    beta = 1.0 / (1.0 + jnp.exp(-fold_blocks(upd.astype(F32))))
    pre = fold_blocks(fade) + bias
    soft = jnp.maximum(pre, 0.0) + jnp.log1p(jnp.exp(-jnp.abs(pre)))
    rate = jnp.exp(jnp.full((NBLK, BLK), loglevel, F32))
    cum = fold_blocks(boost) - rate * soft
    lane = lax.broadcasted_iota(jnp.int32, (NBLK, BLK), 1)
    step = 1
    while step < BLK:
        cum = cum + jnp.where(lane >= step, pltpu.roll(cum, step, 1), 0.0)
        step *= 2
    return beta, cum


def block_inputs(q, k, v, cum_row, beta_row):
    dk = q.shape[-1]
    c_j = jnp.broadcast_to(cum_row, (BLK, BLK))
    c_i = c_j.T
    b_i = jnp.broadcast_to(beta_row, (BLK, BLK)).T
    row = lax.broadcasted_iota(jnp.int32, (BLK, BLK), 0)
    col = lax.broadcasted_iota(jnp.int32, (BLK, BLK), 1)
    decay = jnp.exp(jnp.where(row >= col, c_i - c_j, -1e30))
    e_i = jnp.exp(c_i)
    c_last = jnp.broadcast_to(cum_row[:, BLK - 1 :], (1, BLK))
    qn = normed_rows(q.astype(F32), dk**-0.5)
    kn = normed_rows(k.astype(F32), 1.0)
    kb = kn.astype(BF16)
    both = mm_nt(jnp.concatenate([kb, qn.astype(BF16)], axis=0), kb)
    lower = jnp.where(row > col, -(b_i * both[:BLK] * decay), 0.0)
    intra = (both[BLK:] * decay).astype(BF16)
    right = jnp.concatenate([v.astype(F32) * b_i, kn * (b_i * e_i)[:, :dk]], axis=1)
    tail = kn * jnp.exp(c_last - c_i)[:, :dk]
    return dict(
        lower=lower,
        intra=intra,
        right=right,
        tail=tail.T.astype(BF16),
        query=qn * e_i[:, :dk],
        keep=jnp.exp(c_last),
    )


def inverses(lowers):
    powers = [n.astype(BF16) for n in lowers]
    extra = list(lowers)
    power = [mm(p, p) for p in powers]
    for level in range(1, 7):
        pb = [p.astype(BF16) for p in power]
        if level < 6:
            wide = [
                mm(p, jnp.concatenate([e.astype(BF16), p], axis=1)) for p, e in zip(pb, extra)
            ]
            extra = [e + p + w[:, :BLK] for e, p, w in zip(extra, power, wide)]
            power = [w[:, BLK:] for w in wide]
        else:
            extra = [e + p + mm(q, e) for e, p, q in zip(extra, power, pb)]
    return extra


def local_kernel(
    q1, k1, q2, k2, vals, upd, fade, boost, level, bias,
    r1, r2, o1, o2, pay,
    beta_s, cum_s, keep_s, qd1, qd2, loc1, loc2, add1, add2,
):
    for h in range(2):
        beta, cum = gate_rows(upd[h], fade[h], boost[h], level[h, 0], bias[h, 0])
        beta_s[h * NBLK : (h + 1) * NBLK, :] = beta
        cum_s[h * NBLK : (h + 1) * NBLK, :] = cum

    def parts(it, carry):
        todo = [(h, 2 * it + j) for j in range(2) for h in range(2)]
        ins = []
        for h, n in todo:
            rows = pl.ds(pl.multiple_of(n * BLK, BLK), BLK)
            q, k = (q1, k1) if h == 0 else (q2, k2)
            ins.append(
                block_inputs(
                    q[rows, :],
                    k[rows, :],
                    vals[rows, h * BLK : (h + 1) * BLK],
                    cum_s[pl.ds(h * NBLK + n, 1), :],
                    beta_s[pl.ds(h * NBLK + n, 1), :],
                )
            )
        extra = inverses([i["lower"] for i in ins])
        for (h, n), i, e in zip(todo, ins, extra):
            dk = (128, 64)[h]
            solved = (i["right"] + mm(e, i["right"])).astype(BF16)
            made = mm(jnp.concatenate([i["intra"], i["tail"]], axis=0), solved)
            qd, loc, add = ((qd1, loc1, add1), (qd2, loc2, add2))[h]
            qd[n, :BLK, :] = (i["query"] - made[:BLK, BLK:]).astype(BF16)
            qd[n, BLK:, :] = (-made[BLK:, BLK:]).astype(BF16)
            loc[n] = made[:BLK, :BLK]
            add[n] = made[BLK:, :BLK]
            keep_s[pl.ds(h * NBLK + n, 1), :] = i["keep"]
        return carry

    lax.fori_loop(0, NBLK // 2, parts, 0)

    def eye(dk):
        return (
            lax.broadcasted_iota(jnp.int32, (dk, dk), 0)
            == lax.broadcasted_iota(jnp.int32, (dk, dk), 1)
        ).astype(F32)

    def chain(n, carry):
        rows = pl.ds(pl.multiple_of(n * BLK, BLK), BLK)
        out = []
        for h, (state, total) in enumerate(carry):
            dk = (128, 64)[h]
            qd, loc, add = ((qd1, loc1, add1), (qd2, loc2, add2))[h]
            r, o = ((r1, o1), (r2, o2))[h]
            made = mm(qd[n], state)
            o[rows, :] = loc[n] + made[:BLK, :BLK]
            r[rows, :] = made[:BLK, BLK:].astype(BF16)
            keep = keep_s[pl.ds(h * NBLK + n, 1), :]
            moved = made[BLK:]
            new_a = state[:, :BLK] * keep + moved[:, :BLK] + add[n]
            new_p = state[:, BLK:] * keep[:, :dk] + moved[:, BLK:]
            out.append((jnp.concatenate([new_a, new_p], axis=1), total * keep))
        return tuple(out)

    start = tuple(
        (jnp.concatenate([jnp.zeros((dk, BLK), F32), eye(dk)], axis=1), jnp.ones((1, BLK), F32))
        for dk in (128, 64)
    )
    (s1, g1), (s2, g2) = lax.fori_loop(0, NBLK, chain, start)
    pay[0:128, :] = (s1[:, BLK:] - eye(128) * g1).astype(BF16)
    pay[128:256, :] = s1[:, :BLK].astype(BF16)
    pay[256:320, :] = s2[:, :BLK].astype(BF16)
    row = lax.broadcasted_iota(jnp.int32, (64, 64), 0)
    hi1, hi2 = g1.astype(BF16).astype(F32), g2.astype(BF16).astype(F32)
    scal = jnp.where(row == 0, hi1[:, :64], 0.0)
    scal = scal + jnp.where(row == 1, (g1 - hi1)[:, :64], 0.0)
    scal = scal + jnp.where(row == 2, hi2[:, :64], 0.0)
    scal = scal + jnp.where(row == 3, (g2 - hi2)[:, :64], 0.0)
    d2 = s2[:, BLK:] - eye(64) * g2[:, :64]
    pay[320:384, :] = jnp.concatenate([d2, scal], axis=1).astype(BF16)


def local_recurrence(q1, k1, q2, k2, vals, upd, fade, boost, level, bias):
    vm = pl.BlockSpec(memory_space=pltpu.VMEM)
    sm = pl.BlockSpec(memory_space=pltpu.SMEM)
    return pl.pallas_call(
        local_kernel,
        out_shape=(
            jax.ShapeDtypeStruct((1024, 128), BF16),
            jax.ShapeDtypeStruct((1024, 64), BF16),
            jax.ShapeDtypeStruct((1024, 128), F32),
            jax.ShapeDtypeStruct((1024, 128), F32),
            jax.ShapeDtypeStruct((384, 128), BF16),
        ),
        in_specs=[vm] * 8 + [sm] * 2,
        out_specs=[vm] * 5,
        scratch_shapes=[
            pltpu.VMEM((2 * NBLK, BLK), F32),
            pltpu.VMEM((2 * NBLK, BLK), F32),
            pltpu.VMEM((2 * NBLK, BLK), F32),
            pltpu.VMEM((NBLK, 256, 128), BF16),
            pltpu.VMEM((NBLK, 192, 64), BF16),
            pltpu.VMEM((NBLK, BLK, BLK), F32),
            pltpu.VMEM((NBLK, BLK, BLK), F32),
            pltpu.VMEM((NBLK, 128, BLK), F32),
            pltpu.VMEM((NBLK, 64, BLK), F32),
        ],
        cost_estimate=pl.CostEstimate(
            flops=2_000_000_000, bytes_accessed=4_000_000, transcendentals=1_000_000
        ),
    )(q1, k1, q2, k2, vals, upd, fade, boost, level, bias)


def split_pay(pay):
    p = pay.astype(F32)
    g1 = p[320, 64] + p[321, 64]
    g2 = p[322, 64] + p[323, 64]
    return (p[:128], p[128:256], g1), (p[320:, :64], p[256:320], g2)


def join_pay(one, two):
    (d1, a1, g1), (d2, a2, g2) = one, two
    hi1, hi2 = lax.reduce_precision(g1, 8, 7), lax.reduce_precision(g2, 8, 7)
    scal = jnp.stack([hi1, g1 - hi1, hi2, g2 - hi2])
    scal = jnp.pad(jnp.broadcast_to(scal[:, None], (4, 64)), ((0, 60), (0, 0)))
    low = jnp.concatenate([d2, scal], axis=1)
    return jnp.concatenate([d1, a1, a2, low], axis=0).astype(BF16)


def after(earlier, later):
    d0, a0, g0 = earlier
    d1, a1, g1 = later
    return (g1 * d0 + g0 * d1 + mm(d1, d0), g1 * a0 + a1 + mm(d1, a0), g0 * g1)


def applied(later, state):
    d, a, g = later
    return g * state + a + mm(d, state)


def incoming_states(pay):
    y, z = lax.axis_index("sp_1"), lax.axis_index("sp_0")
    row = lax.all_gather(pay, "sp_1")
    members = [split_pay(row[i]) for i in range(4)]
    whole = members[0]
    for m in members[1:]:
        whole = tuple(after(e, l) for e, l in zip(whole, m))
    rows = lax.all_gather(join_pay(*whole), "sp_0")
    states = [jnp.zeros((128, 128), F32), jnp.zeros((64, 128), F32)]
    for i in range(3):
        states = [
            jnp.where(i < z, applied(m, s), s) for m, s in zip(split_pay(rows[i]), states)
        ]
    for i in range(3):
        states = [jnp.where(i < y, applied(m, s), s) for m, s in zip(members[i], states)]
    return states


def finished_head(local, reads, state, gate_cols, coef):
    out = local + mm(reads, state)
    scaled = out * lax.rsqrt(jnp.mean(out * out, axis=-1, keepdims=True) + EPSILON) * coef
    return (scaled * jax.nn.silu(gate_cols.astype(F32))).astype(BF16)


MESH = pl.DeviceIdType.MESH
WIDTH = 2048
UNITS = 768


def ring_places():
    me = lax.axis_index("tp")
    x, core = me // 2, me % 2
    right = ((x + 1) % 4) * 2 + core
    left = ((x + 3) % 4) * 2 + core
    far = ((x + 2) % 4) * 2 + core
    return me, x, core, x * 2 + 1 - core, right, left, far


def mixer_kernel(
    normed, skip, taps, weights,
    out,
    feat, wgu, wdn, low, hid, acc, d2d_out, d2d_in, far_out, msg_r, msg_l, far_in, in_l, in_r,
    load_sem, send_sem, recv_sem,
):
    me, x, core, mate, right, left, far = ring_places()
    z, y = lax.axis_index("sp_0"), lax.axis_index("sp_1")
    place = z * 4 + y
    after_z, after_y = ((place + 1) % 16) // 4, (place + 1) % 4
    prior_z, prior_y = ((place + 15) % 16) // 4, (place + 15) % 4
    to_mate, to_right, to_left = {"tp": mate}, {"tp": right}, {"tp": left}
    to_next = {"sp_0": after_z, "sp_1": after_y}
    to_prior = {"sp_0": prior_z, "sp_1": prior_y}

    load_gu = pltpu.make_async_copy(weights.at[:, 0 : 2 * UNITS], wgu, load_sem.at[0])
    load_dn = pltpu.make_async_copy(weights.at[:, 2 * UNITS :], wdn, load_sem.at[1])
    load_gu.start()
    load_dn.start()

    barrier = pltpu.get_barrier_semaphore()
    for peer in (to_mate, to_right, to_left, to_next, to_prior):
        pl.semaphore_signal(barrier, inc=1, device_id=peer, device_id_type=MESH)
    pl.semaphore_wait(barrier, 5)

    def send(k, src, dst, peer):
        return pltpu.make_async_remote_copy(
            src_ref=src, dst_ref=dst, send_sem=send_sem.at[k], recv_sem=recv_sem.at[k],
            device_id=peer, device_id_type=MESH,
        )

    def shard(i, first=0, count=128):
        return feat.at[pl.ds(pl.multiple_of(i * 128 + first, 64), count), :]

    half_a, half_b = normed.at[0:64, :], normed.at[64:128, :]
    own_mate = send(0, normed, shard(me), to_mate)
    own = [
        send(1, half_a, shard(me, 0, 64), to_right),
        send(3, half_b, shard(me, 64, 64), to_left),
        send(2, half_b, shard(me, 64, 64), to_right),
        send(4, half_a, shard(me, 0, 64), to_left),
    ]
    own_mate.start()
    for c in own:
        c.start()
    a_right, b_left, b_right, a_left = own
    fwd_a = send(5, shard(left, 0, 64), shard(left, 0, 64), to_right)
    fwd_b = send(6, shard(right, 64, 64), shard(right, 64, 64), to_left)
    mate_l = send(7, shard(left), shard(left), to_mate)
    mate_r = send(8, shard(right), shard(right), to_mate)
    mate_fa = send(9, shard(far, 0, 64), shard(far, 0, 64), to_mate)
    mate_fb = send(10, shard(far, 64, 64), shard(far, 64, 64), to_mate)
    halo_rows = low.at[pl.ds(1024, 16), :]
    halo = send(11, halo_rows, low.at[pl.ds(0, 16), :], to_next)

    feat[pl.ds(pl.multiple_of(me * 128, 128), 128), :] = normed[...]

    def gate_up(pair):
        rows = pl.ds(pl.multiple_of(pair * 256, 256), 256)
        put = pl.ds(pl.multiple_of(pair * 256 + 16, 16), 256)

        def tile(j, carry):
            cols = pl.ds(pl.multiple_of(j * 256, 256), 256)
            low[put, cols] = mm(feat[rows, :], wgu[:, cols]).astype(BF16)
            return carry

        lax.fori_loop(0, 6, tile, 0)

        @pl.when(pair == 3)
        def _():
            halo.start()

    load_gu.wait()
    own_mate.wait_recv()
    gate_up(x)
    a_right.wait_recv()
    fwd_a.start()
    b_left.wait_recv()
    fwd_b.start()
    b_right.wait_recv()
    mate_l.start()
    a_left.wait_recv()
    mate_r.start()
    mate_r.wait_recv()
    gate_up((x + 1) % 4)
    mate_l.wait_recv()
    gate_up((x + 3) % 4)
    fwd_a.wait_recv()
    mate_fa.start()
    fwd_b.wait_recv()
    mate_fb.start()
    mate_fa.wait_recv()
    mate_fb.wait_recv()
    gate_up((x + 2) % 4)
    load_dn.wait()
    halo.wait_recv()

    @pl.when(place == 0)
    def _():
        low[0:16, :] = jnp.zeros((16, 2 * UNITS), BF16)

    def conv(cols, pair, side):
        rows = pl.ds(pl.multiple_of(pair * 256, 256), 272)
        lows = low[rows, pl.ds(pl.multiple_of(cols + side * UNITS, 128), 128)].astype(F32)
        span = pl.ds(pl.multiple_of(cols, 128), 128)
        t = [taps[j, side : side + 1, span].astype(F32) for j in range(3)]
        total = t[0] * pltpu.roll(lows, 2, 0) + t[1] * pltpu.roll(lows, 1, 0) + t[2] * lows
        return total[16:]

    def down(k, pair):
        def mix(j, carry):
            g = conv(j * 128, pair, 0)
            u = conv(j * 128, pair, 1)
            span = pl.ds(pl.multiple_of(j * 128, 128), 128)
            hid[:, span] = (g / (1.0 + jnp.exp(-g)) * u).astype(BF16)
            return carry

        lax.fori_loop(0, 6, mix, 0)
        mine = pl.ds(pl.multiple_of(core * 128, 128), 128)
        other = pl.ds(pl.multiple_of((1 - core) * 128, 128), 128)

        def tile(j, carry):
            span = pl.ds(pl.multiple_of(j * 256, 256), 256)
            both = jnp.concatenate([hid[mine, :], hid[other, :]], axis=0)
            made = mm_nt(both, wdn[span, :])
            acc[k, :, span] = made[:128]
            d2d_out[k, :, span] = made[128:].astype(BF16)
            return carry

        lax.fori_loop(0, 8, tile, 0)
        pair_sum = send(12 + k, d2d_out.at[k], d2d_in.at[k], to_mate)
        pair_sum.start()
        return pair_sum

    far_a = send(16, far_out.at[0:64, :], far_in.at[0:64, :], to_right)
    far_b = send(17, far_out.at[64:128, :], far_in.at[64:128, :], to_left)
    r_b = send(18, msg_r.at[64:128, :], in_l.at[64:128, :], to_right)
    r_a = send(19, msg_r.at[0:64, :], in_l.at[0:64, :], to_right)
    l_a = send(20, msg_l.at[0:64, :], in_r.at[0:64, :], to_left)
    l_b = send(21, msg_l.at[64:128, :], in_r.at[64:128, :], to_left)

    d_far = down(0, (x + 2) % 4)
    d_right = down(1, (x + 1) % 4)
    d_far.wait_recv()
    far_out[...] = (acc[0] + d2d_in[0].astype(F32)).astype(BF16)
    far_a.start()
    far_b.start()
    d_left = down(2, (x + 3) % 4)
    d_right.wait_recv()
    msg_r[64:128, :] = (acc[1, 64:128, :] + d2d_in[1, 64:128, :].astype(F32)).astype(BF16)
    r_b.start()
    d_left.wait_recv()
    msg_l[0:64, :] = (acc[2, 0:64, :] + d2d_in[2, 0:64, :].astype(F32)).astype(BF16)
    l_a.start()
    d_own = down(3, x)
    far_a.wait_recv()
    msg_r[0:64, :] = (
        acc[1, 0:64, :] + d2d_in[1, 0:64, :].astype(F32) + far_in[0:64, :].astype(F32)
    ).astype(BF16)
    r_a.start()
    far_b.wait_recv()
    msg_l[64:128, :] = (
        acc[2, 64:128, :] + d2d_in[2, 64:128, :].astype(F32) + far_in[64:128, :].astype(F32)
    ).astype(BF16)
    l_b.start()
    d_own.wait_recv()
    acc[3] = acc[3] + d2d_in[3].astype(F32) + skip[...]
    for c in (r_b, l_a, r_a, l_b):
        c.wait_recv()
    out[...] = (acc[3] + in_l[...].astype(F32) + in_r[...].astype(F32)).astype(BF16)

    for c in (own_mate, *own, fwd_a, fwd_b, mate_l, mate_r, mate_fa, mate_fb, halo):
        c.wait_send()
    for c in (d_far, d_right, d_left, d_own, far_a, far_b, r_b, r_a, l_a, l_b):
        c.wait_send()


def channel_mixer(normed, skip, taps, weights):
    vm = pl.BlockSpec(memory_space=pltpu.VMEM)
    return pl.pallas_call(
        mixer_kernel,
        out_shape=jax.ShapeDtypeStruct((128, WIDTH), BF16),
        in_specs=[vm, vm, vm, pl.BlockSpec(memory_space=pl.ANY)],
        out_specs=vm,
        scratch_shapes=[
            pltpu.VMEM((1024, WIDTH), BF16),
            pltpu.VMEM((WIDTH, 2 * UNITS), BF16),
            pltpu.VMEM((WIDTH, UNITS), BF16),
            pltpu.VMEM((1040, 2 * UNITS), BF16),
            pltpu.VMEM((256, UNITS), BF16),
            pltpu.VMEM((4, 128, WIDTH), F32),
            pltpu.VMEM((4, 128, WIDTH), BF16),
            pltpu.VMEM((4, 128, WIDTH), BF16),
            pltpu.VMEM((128, WIDTH), BF16),
            pltpu.VMEM((128, WIDTH), BF16),
            pltpu.VMEM((128, WIDTH), BF16),
            pltpu.VMEM((128, WIDTH), BF16),
            pltpu.VMEM((128, WIDTH), BF16),
            pltpu.VMEM((128, WIDTH), BF16),
            pltpu.SemaphoreType.DMA((2,)),
            pltpu.SemaphoreType.DMA((22,)),
            pltpu.SemaphoreType.DMA((22,)),
        ],
        compiler_params=pltpu.CompilerParams(
            collective_id=1, has_side_effects=True, vmem_limit_bytes=60 * 1024 * 1024
        ),
        cost_estimate=pl.CostEstimate(
            flops=10_000_000_000, bytes_accessed=12_000_000, transcendentals=1_000_000
        ),
    )(normed, skip, taps, weights)


def per_device(
    arriving_hidden_state,
    former_request_vectors,
    former_match_vectors,
    latter_request_vectors,
    latter_match_vectors,
    stored_vectors_both,
    closing_valve_operands,
    update_level_before_squash,
    fading_data_input,
    sparse_fading_boost,
    unitwise_fading_loglevel,
    fading_constant_term,
    unitwise_normalizer_coef,
    emission_map_weights,
    channel_normalizer_coef,
    switching_channel_map,
    broadening_channel_map,
    timewise_convolve_tapvalues,
    narrowing_map_weights_in,
):
    gathered = lax.all_gather(
        jnp.concatenate(
            [switching_channel_map, broadening_channel_map, narrowing_map_weights_in], axis=1
        ),
        SP,
        axis=0,
        tiled=True,
    )
    vals = stored_vectors_both.reshape(-1, 256)
    r1, r2, o1, o2, pay = local_recurrence(
        former_request_vectors,
        former_match_vectors,
        latter_request_vectors,
        latter_match_vectors,
        vals,
        update_level_before_squash,
        fading_data_input,
        sparse_fading_boost,
        unitwise_fading_loglevel,
        fading_constant_term,
    )
    s1, s2 = incoming_states(pay)
    linear_attend = jnp.stack(
        [
            finished_head(o1, r1, s1, closing_valve_operands[:, 0], unitwise_normalizer_coef),
            finished_head(o2, r2, s2, closing_valve_operands[:, 1], unitwise_normalizer_coef),
        ],
        axis=1,
    )
    arrived = lax.all_to_all(linear_attend, "tp", split_axis=0, concat_axis=2, tiled=True)
    row_count = arrived.shape[0]
    skip_stream = arriving_hidden_state.astype(jnp.float32) + jnp.dot(
        arrived.reshape(row_count, -1), emission_map_weights, preferred_element_type=jnp.float32
    )
    normed = (
        skip_stream
        * lax.rsqrt(jnp.mean(skip_stream * skip_stream, axis=-1, keepdims=True) + EPSILON)
        * channel_normalizer_coef
    ).astype(jnp.bfloat16)
    return channel_mixer(normed, skip_stream, timewise_convolve_tapvalues, gathered)


def solution(mesh):
    torus = Mesh(mesh.devices.reshape(4, 4, mesh.shape["tp"]), ("sp_0", "sp_1", "tp"))
    return jax.shard_map(
        per_device,
        mesh=torus,
        in_specs=(
            P(SP_TP, None),
            P(SP, "tp"),
            P(SP, "tp"),
            P(SP, "tp"),
            P(SP, "tp"),
            P(SP, None, "tp"),
            P(SP, None, "tp"),
            P(None, "tp", SP),
            P(None, "tp", SP),
            P(None, "tp", SP),
            P(None, "tp"),
            P(None, "tp"),
            P(),
            P(),
            P(),
            P(SP, "tp"),
            P(SP, "tp"),
            P(None, None, "tp"),
            P(SP, "tp"),
        ),
        out_specs=P(SP_TP, None),
        check_vma=False,
    )
```

```python
import jax
import jax.numpy as jnp
from jax import lax
from jax.experimental import pallas as pl
from jax.experimental.pallas import tpu as pltpu
from jax.sharding import Mesh
from jax.sharding import PartitionSpec as P

SP = ("sp_0", "sp_1")
SP_TP = ("sp_0", "sp_1", "tp")
MESH = pl.DeviceIdType.MESH
WIDTH = 2048
UNITS = 768

BLK = 128
NBLK = 8
EPSILON = 1e-06
F32 = jnp.float32
BF16 = jnp.bfloat16


def mm(a, b):
    return jnp.dot(a.astype(BF16), b.astype(BF16), preferred_element_type=F32)


def mm_nt(a, b):
    return lax.dot_general(
        a.astype(BF16), b.astype(BF16), (((1,), (1,)), ((), ())), preferred_element_type=F32
    )


def normed_rows(x, scale):
    return x * (lax.rsqrt(jnp.sum(x * x, axis=-1, keepdims=True) + EPSILON) * scale)


def fold_blocks(row):
    return jnp.concatenate([row[:, i * BLK : (i + 1) * BLK] for i in range(NBLK)], axis=0)


def gate_rows(upd, fade, boost, loglevel, bias):
    beta = 1.0 / (1.0 + jnp.exp(-fold_blocks(upd.astype(F32))))
    pre = fold_blocks(fade) + bias
    soft = jnp.maximum(pre, 0.0) + jnp.log1p(jnp.exp(-jnp.abs(pre)))
    rate = jnp.exp(jnp.full((NBLK, BLK), loglevel, F32))
    cum = fold_blocks(boost) - rate * soft
    lane = lax.broadcasted_iota(jnp.int32, (NBLK, BLK), 1)
    step = 1
    while step < BLK:
        cum = cum + jnp.where(lane >= step, pltpu.roll(cum, step, 1), 0.0)
        step *= 2
    return beta, cum


def block_inputs(q, k, v, cum_row, beta_row):
    dk = q.shape[-1]
    c_j = jnp.broadcast_to(cum_row, (BLK, BLK))
    c_i = c_j.T
    b_i = jnp.broadcast_to(beta_row, (BLK, BLK)).T
    row = lax.broadcasted_iota(jnp.int32, (BLK, BLK), 0)
    col = lax.broadcasted_iota(jnp.int32, (BLK, BLK), 1)
    decay = jnp.exp(jnp.where(row >= col, c_i - c_j, -1e30))
    e_i = jnp.exp(c_i)
    c_last = jnp.broadcast_to(cum_row[:, BLK - 1 :], (1, BLK))
    qn = normed_rows(q.astype(F32), dk**-0.5)
    kn = normed_rows(k.astype(F32), 1.0)
    kb = kn.astype(BF16)
    both = mm_nt(jnp.concatenate([kb, qn.astype(BF16)], axis=0), kb)
    lower = jnp.where(row > col, -(b_i * both[:BLK] * decay), 0.0)
    intra = (both[BLK:] * decay).astype(BF16)
    right = jnp.concatenate([v.astype(F32) * b_i, kn * (b_i * e_i)[:, :dk]], axis=1)
    tail = kn * jnp.exp(c_last - c_i)[:, :dk]
    return dict(
        lower=lower,
        intra=intra,
        right=right,
        tail=tail.T.astype(BF16),
        query=qn * e_i[:, :dk],
        keep=jnp.exp(c_last),
    )


def inverses(lowers):
    powers = [n.astype(BF16) for n in lowers]
    extra = list(lowers)
    power = [mm(p, p) for p in powers]
    for level in range(1, 7):
        pb = [p.astype(BF16) for p in power]
        if level < 6:
            wide = [
                mm(p, jnp.concatenate([e.astype(BF16), p], axis=1)) for p, e in zip(pb, extra)
            ]
            extra = [e + p + w[:, :BLK] for e, p, w in zip(extra, power, wide)]
            power = [w[:, BLK:] for w in wide]
        else:
            extra = [e + p + mm(q, e) for e, p, q in zip(extra, power, pb)]
    return extra


def ring_places():
    me = lax.axis_index("tp")
    x, core = me // 2, me % 2
    right = ((x + 1) % 4) * 2 + core
    left = ((x + 3) % 4) * 2 + core
    far = ((x + 2) % 4) * 2 + core
    return me, x, core, x * 2 + 1 - core, right, left, far


def read_maps(pays, i):
    low = pays[i, 320:384, :].astype(F32)
    g1 = low[0:1, 64:65] + low[1:2, 64:65]
    g2 = low[2:3, 64:65] + low[3:4, 64:65]
    one = (pays[i, 0:128, :], pays[i, 128:256, :].astype(F32), g1)
    two = (pays[i, 320:384, :][:, :64], pays[i, 256:320, :].astype(F32), g2)
    return one, two


def after(earlier, later):
    d0, a0, g0 = earlier
    d1, a1, g1 = later
    made = mm(d1, jnp.concatenate([a0, d0], axis=1))
    return (
        d0 * g1 + d1.astype(F32) * g0 + made[:, BLK:],
        a0 * g1 + a1 + made[:, :BLK],
        g0 * g1,
    )


def write_maps(pays, i, one, two):
    (d1, a1, g1), (d2, a2, g2) = one, two
    row = lax.broadcasted_iota(jnp.int32, (64, 64), 0)
    hi1, hi2 = g1.astype(BF16).astype(F32), g2.astype(BF16).astype(F32)
    scal = jnp.where(row == 0, jnp.broadcast_to(hi1, (64, 64)), 0.0)
    scal = scal + jnp.where(row == 1, jnp.broadcast_to(g1 - hi1, (64, 64)), 0.0)
    scal = scal + jnp.where(row == 2, jnp.broadcast_to(hi2, (64, 64)), 0.0)
    scal = scal + jnp.where(row == 3, jnp.broadcast_to(g2 - hi2, (64, 64)), 0.0)
    pays[i, 0:128, :] = d1.astype(BF16)
    pays[i, 128:256, :] = a1.astype(BF16)
    pays[i, 256:320, :] = a2.astype(BF16)
    pays[i, 320:384, :] = jnp.concatenate([d2, scal], axis=1).astype(BF16)


def layer_kernel(
    q1, k1, q2, k2, vals, gates, upd, fade, boost, level, bias, norm_coef,
    emission, chan_coef, hidden, w_gate, w_up, w_down, taps,
    out,
    beta_s, cum_s, keep_s, qd1, qd2, loc1, loc2, add1, add2, vf, gf, r1, r2, o1, o2,
    pays, row_pays, heads, arrived, emit_w, skip, normed, wall,
    feat, low, hid, acc, d2d_out, d2d_in, far_out, msg_r, msg_l, far_in, in_l, in_r,
    load_sem, send_sem, recv_sem, wsend, wrecv,
):
    me, x, core, mate, right, left, far = ring_places()
    z, y = lax.axis_index("sp_0"), lax.axis_index("sp_1")
    place = z * 4 + y
    after_z, after_y = ((place + 1) % 16) // 4, (place + 1) % 4
    prior_z, prior_y = ((place + 15) % 16) // 4, (place + 15) % 4
    to_mate, to_right, to_left = {"tp": mate}, {"tp": right}, {"tp": left}
    to_next = {"sp_0": after_z, "sp_1": after_y}
    to_prior = {"sp_0": prior_z, "sp_1": prior_y}

    home = pl.ds(pl.multiple_of(place * 128, 128), 128)
    loads = [
        pltpu.make_async_copy(w_gate, wall.at[home, 0:UNITS], load_sem.at[0]),
        pltpu.make_async_copy(w_up, wall.at[home, UNITS : 2 * UNITS], load_sem.at[1]),
        pltpu.make_async_copy(w_down, wall.at[home, 2 * UNITS :], load_sem.at[2]),
        pltpu.make_async_copy(emission, emit_w, load_sem.at[3]),
    ]
    for c in loads:
        c.start()

    step = 1 - 2 * core
    at = (y, z)
    names = ("sp_1", "sp_0")
    ahead = ((y + step + 4) % 4, (z + step + 4) % 4)
    behind = ((y - step + 4) % 4, (z - step + 4) % 4)
    across = ((y + 2) % 4, (z + 2) % 4)

    barrier = pltpu.get_barrier_semaphore()
    peers = [{"tp": (me + i) % 8} for i in range(1, 8)]
    peers += [{names[d]: n[d]} for d in range(2) for n in (ahead, behind)]
    peers += [to_next, to_prior]
    for peer in peers:
        pl.semaphore_signal(barrier, inc=1, device_id=peer, device_id_type=MESH)

    def ring_copy(sems, k, kind, ref_at, dim):
        src = ref_at(behind[dim] if kind == 2 else at[dim])
        goal = behind[dim] if kind == 1 else ahead[dim]
        return pltpu.make_async_remote_copy(
            src_ref=src, dst_ref=src, send_sem=sems[0].at[k], recv_sem=sems[1].at[k],
            device_id={names[dim]: goal}, device_id_type=MESH,
        )

    def weight_block(along_y, along_z, kind, chunk):
        first = (along_z * 4 + along_y) * 128 + 64 * kind
        cols = (slice(0, 2 * UNITS), slice(2 * UNITS, 3 * UNITS))[chunk]
        return wall.at[pl.ds(pl.multiple_of(first, 64), 64), cols]

    def first_ring(chunk, kind, what):
        def ref_at(i):
            return weight_block(i, z, 0, chunk) if kind == 0 else weight_block(y, i, 1, chunk)

        return ring_copy((wsend, wrecv), (chunk * 2 + kind) * 15 + what, what, ref_at, kind)

    def second_ring(chunk, kind, piece, what):
        other = (at[kind], behind[kind], ahead[kind], across[kind])[piece]

        def ref_at(i):
            if kind == 0:
                return weight_block(other, i, 0, chunk)
            return weight_block(i, other, 1, chunk)

        k = (chunk * 2 + kind) * 15 + 3 + piece * 3 + what
        return ring_copy((wsend, wrecv), k, what, ref_at, 1 - kind)

    pl.semaphore_wait(barrier, 13)
    for chunk in range(2):
        for c in (loads[:2], loads[2:3])[chunk]:
            c.wait()
        for kind in range(2):
            first_ring(chunk, kind, 0).start()
            first_ring(chunk, kind, 1).start()

    vf[...] = vals[...].astype(F32)
    gf[...] = gates[...].astype(F32)
    for h in range(2):
        beta, cum = gate_rows(upd[...].astype(F32)[h : h + 1], fade[h], boost[h], level[0, h], bias[0, h])
        beta_s[h * NBLK : (h + 1) * NBLK, :] = beta
        cum_s[h * NBLK : (h + 1) * NBLK, :] = cum

    def parts(it, carry):
        todo = [(h, 2 * it + j) for j in range(2) for h in range(2)]
        ins = []
        for h, n in todo:
            rows = pl.ds(pl.multiple_of(n * BLK, BLK), BLK)
            if h == 0:
                q, k = q1[rows, :].astype(F32), k1[rows, :].astype(F32)
            else:
                q, k = q2[:, rows].astype(F32).T, k2[:, rows].astype(F32).T
            ins.append(
                block_inputs(
                    q,
                    k,
                    vf[pl.ds(2 * n * BLK + h, BLK, 2), :],
                    cum_s[pl.ds(h * NBLK + n, 1), :],
                    beta_s[pl.ds(h * NBLK + n, 1), :],
                )
            )
        extra = inverses([i["lower"] for i in ins])
        for (h, n), i, e in zip(todo, ins, extra):
            dk = (128, 64)[h]
            solved = (i["right"] + mm(e, i["right"])).astype(BF16)
            made = mm(jnp.concatenate([i["intra"], i["tail"]], axis=0), solved)
            qd, loc, add = ((qd1, loc1, add1), (qd2, loc2, add2))[h]
            qd[n, :BLK, :] = (i["query"] - made[:BLK, BLK:]).astype(BF16)
            qd[n, BLK:, :] = (-made[BLK:, BLK:]).astype(BF16)
            loc[n] = made[:BLK, :BLK]
            add[n] = made[BLK:, :BLK]
            keep_s[pl.ds(h * NBLK + n, 1), :] = i["keep"]
        return carry

    lax.fori_loop(0, 2, parts, 0)
    for kind in range(2):
        first_ring(0, kind, 0).wait_recv()
        first_ring(0, kind, 2).start()
        second_ring(0, kind, 0, 0).start()
        second_ring(0, kind, 0, 1).start()
    lax.fori_loop(2, NBLK // 2, parts, 0)
    for kind in range(2):
        first_ring(1, kind, 0).wait_recv()
        first_ring(1, kind, 2).start()

    def eye(dk):
        return (
            lax.broadcasted_iota(jnp.int32, (dk, dk), 0)
            == lax.broadcasted_iota(jnp.int32, (dk, dk), 1)
        ).astype(F32)

    def chain(n, carry):
        rows = pl.ds(pl.multiple_of(n * BLK, BLK), BLK)
        out = []
        for h, (state, total) in enumerate(carry):
            dk = (128, 64)[h]
            qd, loc, add = ((qd1, loc1, add1), (qd2, loc2, add2))[h]
            r, o = ((r1, o1), (r2, o2))[h]
            made = mm(qd[n], state)
            o[rows, :] = loc[n] + made[:BLK, :BLK]
            r[rows, :] = made[:BLK, BLK:].astype(BF16)
            keep = keep_s[pl.ds(h * NBLK + n, 1), :]
            moved = made[BLK:]
            new_a = state[:, :BLK] * keep + moved[:, :BLK] + add[n]
            new_p = state[:, BLK:] * keep[:, :dk] + moved[:, BLK:]
            out.append((jnp.concatenate([new_a, new_p], axis=1), total * keep))
        return tuple(out)

    start = tuple(
        (jnp.concatenate([jnp.zeros((dk, BLK), F32), eye(dk)], axis=1), jnp.ones((1, BLK), F32))
        for dk in (128, 64)
    )
    (s1, g1), (s2, g2) = lax.fori_loop(0, NBLK, chain, start)
    write_maps(
        pays,
        y,
        (s1[:, BLK:] - eye(128) * g1, s1[:, :BLK], g1[:, :1]),
        (s2[:, BLK:] - eye(64) * g2[:, :64], s2[:, :BLK], g2[:, :1]),
    )

    def exchange(buf, dim, what):
        sems = (send_sem, recv_sem)
        return ring_copy(sems, 22 + dim * 3 + what, what, lambda i: buf.at[i], dim)

    exchange(pays, 0, 0).start()
    exchange(pays, 0, 1).start()
    for kind in range(2):
        second_ring(0, kind, 0, 0).wait_recv()
    exchange(pays, 0, 0).wait_recv()
    exchange(pays, 0, 2).start()
    for kind in range(2):
        second_ring(0, kind, 0, 2).start()
    exchange(pays, 0, 1).wait_recv()
    exchange(pays, 0, 2).wait_recv()
    whole = read_maps(pays, 0)
    whole = tuple((d.astype(F32), a, g) for d, a, g in whole)
    for i in range(1, 4):
        whole = tuple(after(e, l) for e, l in zip(whole, read_maps(pays, i)))
    write_maps(row_pays, z, *whole)
    exchange(row_pays, 1, 0).start()
    exchange(row_pays, 1, 1).start()
    exchange(row_pays, 1, 0).wait_recv()
    exchange(row_pays, 1, 2).start()
    for kind in range(2):
        first_ring(0, kind, 1).wait_recv()
        first_ring(0, kind, 2).wait_recv()
        for piece in (1, 2, 3):
            second_ring(0, kind, piece, 0).start()
            second_ring(0, kind, piece, 1).start()
    exchange(row_pays, 1, 1).wait_recv()
    exchange(row_pays, 1, 2).wait_recv()

    states = [jnp.zeros((128, BLK), F32), jnp.zeros((64, BLK), F32)]
    for buf, limit in ((row_pays, z), (pays, y)):
        for i in range(3):
            moved = [
                s * g + a + mm(d, s) for (d, a, g), s in zip(read_maps(buf, i), states)
            ]
            states = [jnp.where(i < limit, m, s) for m, s in zip(moved, states)]
    states = [s.astype(BF16) for s in states]

    order = (far, far + 1 - 2 * core, right, right + 1 - 2 * core, left, left + 1 - 2 * core, mate)

    def finish(n):
        rows = pl.ds(pl.multiple_of(n * BLK, BLK), BLK)
        for h in range(2):
            o, r = ((o1, r1), (o2, r2))[h]
            head = o[rows, :] + mm(r[rows, :], states[h])
            scale = lax.rsqrt(jnp.mean(head * head, axis=-1, keepdims=True) + EPSILON)
            g = gf[pl.ds(2 * n * BLK + h, BLK, 2), :]
            made = head * scale * norm_coef[...] * (g / (1.0 + jnp.exp(-g)))
            heads[n, :, h * BLK : (h + 1) * BLK] = made.astype(BF16)

    def hand_out(k):
        return pltpu.make_async_remote_copy(
            src_ref=heads.at[order[k]], dst_ref=arrived.at[me],
            send_sem=send_sem.at[28 + k], recv_sem=recv_sem.at[28 + k],
            device_id={"tp": order[k]}, device_id_type=MESH,
        )

    for k in range(7):
        finish(order[k])
        hand_out(k).start()
    finish(me)
    arrived[me] = heads[me]
    skip[...] = hidden[...].astype(F32)
    loads[3].wait()

    def emit(pair):
        firsts = [arrived[2 * pair + i] for i in range(2)]
        one = jnp.concatenate([f[:, :BLK] for f in firsts], axis=1)
        two = jnp.concatenate([f[:, BLK:] for f in firsts], axis=1)
        upper = pl.ds(pl.multiple_of(pair * 256, 256), 256)
        lower = pl.ds(pl.multiple_of(pair * 256 + 1024, 256), 256)

        def tile(j, carry):
            cols = pl.ds(pl.multiple_of(j * 512, 512), 512)
            skip[:, cols] += mm(one, emit_w[upper, cols]) + mm(two, emit_w[lower, cols])
            return carry

        lax.fori_loop(0, 4, tile, 0)

    hand_out(6).wait_recv()
    emit(x)
    hand_out(2).wait_recv()
    hand_out(3).wait_recv()
    emit((x + 3) % 4)
    hand_out(4).wait_recv()
    hand_out(5).wait_recv()
    emit((x + 1) % 4)
    hand_out(0).wait_recv()
    hand_out(1).wait_recv()
    emit((x + 2) % 4)
    full = skip[...]
    norm = lax.rsqrt(jnp.mean(full * full, axis=-1, keepdims=True) + EPSILON)
    normed[...] = (full * norm * chan_coef[...]).astype(BF16)

    def send(k, src, dst, peer):
        return pltpu.make_async_remote_copy(
            src_ref=src, dst_ref=dst, send_sem=send_sem.at[k], recv_sem=recv_sem.at[k],
            device_id=peer, device_id_type=MESH,
        )

    def shard(i, first=0, count=128):
        return feat.at[pl.ds(pl.multiple_of(i * 128 + first, 64), count), :]

    half_a, half_b = normed.at[0:64, :], normed.at[64:128, :]
    own_mate = send(0, normed, shard(me), to_mate)
    own = [
        send(1, half_a, shard(me, 0, 64), to_right),
        send(3, half_b, shard(me, 64, 64), to_left),
        send(2, half_b, shard(me, 64, 64), to_right),
        send(4, half_a, shard(me, 0, 64), to_left),
    ]
    own_mate.start()
    for c in own:
        c.start()
    a_right, b_left, b_right, a_left = own
    for kind in range(2):
        for piece in (1, 2, 3):
            second_ring(0, kind, piece, 0).wait_recv()
            second_ring(0, kind, piece, 2).start()
        first_ring(1, kind, 1).wait_recv()
        first_ring(1, kind, 2).wait_recv()
        for piece in range(4):
            second_ring(1, kind, piece, 0).start()
            second_ring(1, kind, piece, 1).start()
    fwd_a = send(5, shard(left, 0, 64), shard(left, 0, 64), to_right)
    fwd_b = send(6, shard(right, 64, 64), shard(right, 64, 64), to_left)
    mate_l = send(7, shard(left), shard(left), to_mate)
    mate_r = send(8, shard(right), shard(right), to_mate)
    mate_fa = send(9, shard(far, 0, 64), shard(far, 0, 64), to_mate)
    mate_fb = send(10, shard(far, 64, 64), shard(far, 64, 64), to_mate)
    halo_rows = low.at[pl.ds(1024, 16), :]
    halo = send(11, halo_rows, low.at[pl.ds(0, 16), :], to_next)

    feat[pl.ds(pl.multiple_of(me * 128, 128), 128), :] = normed[...]

    def gate_up(pair):
        rows = pl.ds(pl.multiple_of(pair * 256, 256), 256)
        put = pl.ds(pl.multiple_of(pair * 256 + 16, 16), 256)

        def tile(j, carry):
            cols = pl.ds(pl.multiple_of(j * 256, 256), 256)
            low[put, cols] = mm(feat[rows, :], wall[:, cols]).astype(BF16)
            return carry

        lax.fori_loop(0, 6, tile, 0)

        @pl.when(pair == 3)
        def _():
            halo.start()

    a_right.wait_recv()
    fwd_a.start()
    b_left.wait_recv()
    fwd_b.start()
    for kind in range(2):
        second_ring(0, kind, 0, 1).wait_recv()
        second_ring(0, kind, 0, 2).wait_recv()
        for piece in (1, 2, 3):
            second_ring(0, kind, piece, 1).wait_recv()
            second_ring(0, kind, piece, 2).wait_recv()
    own_mate.wait_recv()
    gate_up(x)
    b_right.wait_recv()
    mate_l.start()
    a_left.wait_recv()
    mate_r.start()
    for kind in range(2):
        for piece in range(4):
            second_ring(1, kind, piece, 0).wait_recv()
            second_ring(1, kind, piece, 2).start()
    mate_r.wait_recv()
    gate_up((x + 1) % 4)
    mate_l.wait_recv()
    gate_up((x + 3) % 4)
    fwd_a.wait_recv()
    mate_fa.start()
    fwd_b.wait_recv()
    mate_fb.start()
    mate_fa.wait_recv()
    mate_fb.wait_recv()
    gate_up((x + 2) % 4)
    for kind in range(2):
        for piece in range(4):
            second_ring(1, kind, piece, 1).wait_recv()
            second_ring(1, kind, piece, 2).wait_recv()
    halo.wait_recv()

    @pl.when(place == 0)
    def _():
        low[0:16, :] = jnp.zeros((16, 2 * UNITS), BF16)

    def conv(cols, pair, side):
        rows = pl.ds(pl.multiple_of(pair * 256, 256), 272)
        lows = low[rows, pl.ds(pl.multiple_of(cols + side * UNITS, 128), 128)].astype(F32)
        span = pl.ds(pl.multiple_of(cols, 128), 128)
        t = [taps[j, side : side + 1, span].astype(F32) for j in range(3)]
        total = t[0] * pltpu.roll(lows, 2, 0) + t[1] * pltpu.roll(lows, 1, 0) + t[2] * lows
        return total[16:]

    def down(k, pair):
        def mix(j, carry):
            g = conv(j * 128, pair, 0)
            u = conv(j * 128, pair, 1)
            span = pl.ds(pl.multiple_of(j * 128, 128), 128)
            hid[:, span] = (g / (1.0 + jnp.exp(-g)) * u).astype(BF16)
            return carry

        lax.fori_loop(0, 6, mix, 0)
        mine = pl.ds(pl.multiple_of(core * 128, 128), 128)
        other = pl.ds(pl.multiple_of((1 - core) * 128, 128), 128)

        def tile(j, carry):
            span = pl.ds(pl.multiple_of(j * 256, 256), 256)
            both = jnp.concatenate([hid[mine, :], hid[other, :]], axis=0)
            made = mm_nt(both, wall[span, 2 * UNITS :])
            acc[k, :, span] = made[:128]
            d2d_out[k, :, span] = made[128:].astype(BF16)
            return carry

        lax.fori_loop(0, 8, tile, 0)
        pair_sum = send(12 + k, d2d_out.at[k], d2d_in.at[k], to_mate)
        pair_sum.start()
        return pair_sum

    far_a = send(16, far_out.at[0:64, :], far_in.at[0:64, :], to_right)
    far_b = send(17, far_out.at[64:128, :], far_in.at[64:128, :], to_left)
    r_b = send(18, msg_r.at[64:128, :], in_l.at[64:128, :], to_right)
    r_a = send(19, msg_r.at[0:64, :], in_l.at[0:64, :], to_right)
    l_a = send(20, msg_l.at[0:64, :], in_r.at[0:64, :], to_left)
    l_b = send(21, msg_l.at[64:128, :], in_r.at[64:128, :], to_left)

    d_far = down(0, (x + 2) % 4)
    d_right = down(1, (x + 1) % 4)
    d_far.wait_recv()
    far_out[...] = (acc[0] + d2d_in[0].astype(F32)).astype(BF16)
    far_a.start()
    far_b.start()
    d_left = down(2, (x + 3) % 4)
    d_right.wait_recv()
    msg_r[64:128, :] = (acc[1, 64:128, :] + d2d_in[1, 64:128, :].astype(F32)).astype(BF16)
    r_b.start()
    d_left.wait_recv()
    msg_l[0:64, :] = (acc[2, 0:64, :] + d2d_in[2, 0:64, :].astype(F32)).astype(BF16)
    l_a.start()
    d_own = down(3, x)
    far_a.wait_recv()
    msg_r[0:64, :] = (
        acc[1, 0:64, :] + d2d_in[1, 0:64, :].astype(F32) + far_in[0:64, :].astype(F32)
    ).astype(BF16)
    r_a.start()
    far_b.wait_recv()
    msg_l[64:128, :] = (
        acc[2, 64:128, :] + d2d_in[2, 64:128, :].astype(F32) + far_in[64:128, :].astype(F32)
    ).astype(BF16)
    l_b.start()
    d_own.wait_recv()
    acc[3] = acc[3] + d2d_in[3].astype(F32) + skip[...]
    for c in (r_b, l_a, r_a, l_b):
        c.wait_recv()
    out[...] = (acc[3] + in_l[...].astype(F32) + in_r[...].astype(F32)).astype(BF16)

    for c in (own_mate, *own, fwd_a, fwd_b, mate_l, mate_r, mate_fa, mate_fb, halo):
        c.wait_send()
    for c in (d_far, d_right, d_left, d_own, far_a, far_b, r_b, r_a, l_a, l_b):
        c.wait_send()
    for dim, buf in ((0, pays), (1, row_pays)):
        for what in range(3):
            exchange(buf, dim, what).wait_send()
    for k in range(7):
        hand_out(k).wait_send()
    for chunk in range(2):
        for kind in range(2):
            for what in range(3):
                first_ring(chunk, kind, what).wait_send()
                for piece in range(4):
                    second_ring(chunk, kind, piece, what).wait_send()


def whole_layer(*args):
    vm = pl.BlockSpec(memory_space=pltpu.VMEM)
    sm = pl.BlockSpec(memory_space=pltpu.SMEM)
    hbm = pl.BlockSpec(memory_space=pl.ANY)
    block = [(128, WIDTH)] * 6
    return pl.pallas_call(
        layer_kernel,
        out_shape=jax.ShapeDtypeStruct((128, WIDTH), BF16),
        in_specs=[vm] * 9 + [sm] * 2 + [vm, hbm, vm, vm, hbm, hbm, hbm, vm],
        out_specs=vm,
        scratch_shapes=[
            *[pltpu.VMEM((2 * NBLK, BLK), F32)] * 3,
            pltpu.VMEM((NBLK, 256, 128), BF16),
            pltpu.VMEM((NBLK, 192, 64), BF16),
            pltpu.VMEM((NBLK, BLK, BLK), F32),
            pltpu.VMEM((NBLK, BLK, BLK), F32),
            pltpu.VMEM((NBLK, 128, BLK), F32),
            pltpu.VMEM((NBLK, 64, BLK), F32),
            pltpu.VMEM((2048, BLK), F32),
            pltpu.VMEM((2048, BLK), F32),
            pltpu.VMEM((1024, 128), BF16),
            pltpu.VMEM((1024, 64), BF16),
            pltpu.VMEM((1024, BLK), F32),
            pltpu.VMEM((1024, BLK), F32),
            pltpu.VMEM((4, 384, 128), BF16),
            pltpu.VMEM((4, 384, 128), BF16),
            pltpu.VMEM((8, 128, 256), BF16),
            pltpu.VMEM((8, 128, 256), BF16),
            pltpu.VMEM((WIDTH, WIDTH), BF16),
            pltpu.VMEM((128, WIDTH), F32),
            pltpu.VMEM((128, WIDTH), BF16),
            pltpu.VMEM((WIDTH, 3 * UNITS), BF16),
            pltpu.VMEM((1024, WIDTH), BF16),
            pltpu.VMEM((1040, 2 * UNITS), BF16),
            pltpu.VMEM((256, UNITS), BF16),
            pltpu.VMEM((4, 128, WIDTH), F32),
            pltpu.VMEM((4, 128, WIDTH), BF16),
            pltpu.VMEM((4, 128, WIDTH), BF16),
            *[pltpu.VMEM(b, BF16) for b in block],
            pltpu.SemaphoreType.DMA((4,)),
            pltpu.SemaphoreType.DMA((35,)),
            pltpu.SemaphoreType.DMA((35,)),
            pltpu.SemaphoreType.DMA((60,)),
            pltpu.SemaphoreType.DMA((60,)),
        ],
        compiler_params=pltpu.CompilerParams(
            collective_id=1, has_side_effects=True, vmem_limit_bytes=62 * 1024 * 1024
        ),
    )(*args)


def per_device(
    arriving_hidden_state,
    former_request_vectors,
    former_match_vectors,
    latter_request_vectors,
    latter_match_vectors,
    stored_vectors_both,
    closing_valve_operands,
    update_level_before_squash,
    fading_data_input,
    sparse_fading_boost,
    unitwise_fading_loglevel,
    fading_constant_term,
    unitwise_normalizer_coef,
    emission_map_weights,
    channel_normalizer_coef,
    switching_channel_map,
    broadening_channel_map,
    timewise_convolve_tapvalues,
    narrowing_map_weights_in,
):
    return whole_layer(
        former_request_vectors,
        former_match_vectors,
        latter_request_vectors.T,
        latter_match_vectors.T,
        stored_vectors_both.reshape(-1, 128),
        closing_valve_operands.reshape(-1, 128),
        update_level_before_squash.reshape(2, -1),
        fading_data_input,
        sparse_fading_boost,
        unitwise_fading_loglevel.reshape(1, 2),
        fading_constant_term.reshape(1, 2),
        unitwise_normalizer_coef.reshape(1, -1),
        emission_map_weights,
        channel_normalizer_coef.reshape(1, -1),
        arriving_hidden_state,
        switching_channel_map,
        broadening_channel_map,
        narrowing_map_weights_in,
        timewise_convolve_tapvalues,
    )


def solution(mesh):
    torus = Mesh(mesh.devices.reshape(4, 4, mesh.shape["tp"]), ("sp_0", "sp_1", "tp"))
    return jax.shard_map(
        per_device,
        mesh=torus,
        in_specs=(
            P(SP_TP, None),
            P(SP, "tp"),
            P(SP, "tp"),
            P(SP, "tp"),
            P(SP, "tp"),
            P(SP, None, "tp"),
            P(SP, None, "tp"),
            P(None, "tp", SP),
            P(None, "tp", SP),
            P(None, "tp", SP),
            P(None, "tp"),
            P(None, "tp"),
            P(),
            P(),
            P(),
            P(SP, "tp"),
            P(SP, "tp"),
            P(None, None, "tp"),
            P(SP, "tp"),
        ),
        out_specs=P(SP_TP, None),
        check_vma=False,
    )
```

```python
import jax
import jax.numpy as jnp
from jax import lax
from jax.experimental import pallas as pl
from jax.experimental.pallas import tpu as pltpu
from jax.sharding import Mesh
from jax.sharding import PartitionSpec as P

SP = ("sp_0", "sp_1")
SP_TP = ("sp_0", "sp_1", "tp")
MESH = pl.DeviceIdType.MESH
WIDTH = 2048
UNITS = 768

BLK = 128
NBLK = 8
EPSILON = 1e-06
F32 = jnp.float32
BF16 = jnp.bfloat16


def mm(a, b):
    return jnp.dot(a.astype(BF16), b.astype(BF16), preferred_element_type=F32)


def mm_nt(a, b):
    return lax.dot_general(
        a.astype(BF16), b.astype(BF16), (((1,), (1,)), ((), ())), preferred_element_type=F32
    )


def normed_rows(x, scale):
    return x * (lax.rsqrt(jnp.sum(x * x, axis=-1, keepdims=True) + EPSILON) * scale)


def fold_blocks(row):
    return jnp.concatenate([row[:, i * BLK : (i + 1) * BLK] for i in range(NBLK)], axis=0)


def gate_rows(upd, fade, boost, loglevel, bias):
    beta = 1.0 / (1.0 + jnp.exp(-fold_blocks(upd.astype(F32))))
    pre = fold_blocks(fade) + bias
    soft = jnp.maximum(pre, 0.0) + jnp.log1p(jnp.exp(-jnp.abs(pre)))
    rate = jnp.exp(jnp.full((NBLK, BLK), loglevel, F32))
    cum = fold_blocks(boost) - rate * soft
    lane = lax.broadcasted_iota(jnp.int32, (NBLK, BLK), 1)
    step = 1
    while step < BLK:
        cum = cum + jnp.where(lane >= step, pltpu.roll(cum, step, 1), 0.0)
        step *= 2
    return beta, cum


def block_inputs(q, k, v, cum_row, beta_row):
    dk = q.shape[-1]
    c_j = jnp.broadcast_to(cum_row, (BLK, BLK))
    c_i = c_j.T
    b_i = jnp.broadcast_to(beta_row, (BLK, BLK)).T
    row = lax.broadcasted_iota(jnp.int32, (BLK, BLK), 0)
    col = lax.broadcasted_iota(jnp.int32, (BLK, BLK), 1)
    decay = jnp.exp(jnp.where(row >= col, c_i - c_j, -1e30))
    e_i = jnp.exp(c_i)
    c_last = jnp.broadcast_to(cum_row[:, BLK - 1 :], (1, BLK))
    qn = normed_rows(q.astype(F32), dk**-0.5)
    kn = normed_rows(k.astype(F32), 1.0)
    kb = kn.astype(BF16)
    both = mm_nt(jnp.concatenate([kb, qn.astype(BF16)], axis=0), kb)
    lower = jnp.where(row > col, -(b_i * both[:BLK] * decay), 0.0)
    intra = (both[BLK:] * decay).astype(BF16)
    right = jnp.concatenate([v.astype(F32) * b_i, kn * (b_i * e_i)[:, :dk]], axis=1)
    tail = kn * jnp.exp(c_last - c_i)[:, :dk]
    return dict(
        lower=lower,
        intra=intra,
        right=right,
        tail=tail.T.astype(BF16),
        query=qn * e_i[:, :dk],
        keep=jnp.exp(c_last),
    )


def inverses(lowers):
    powers = [n.astype(BF16) for n in lowers]
    extra = list(lowers)
    power = [mm(p, p) for p in powers]
    for level in range(1, 7):
        pb = [p.astype(BF16) for p in power]
        if level < 6:
            wide = [
                mm(p, jnp.concatenate([e.astype(BF16), p], axis=1)) for p, e in zip(pb, extra)
            ]
            extra = [e + p + w[:, :BLK] for e, p, w in zip(extra, power, wide)]
            power = [w[:, BLK:] for w in wide]
        else:
            extra = [e + p + mm(q, e) for e, p, q in zip(extra, power, pb)]
    return extra


def ring_places():
    me = lax.axis_index("tp")
    x, core = me // 2, me % 2
    right = ((x + 1) % 4) * 2 + core
    left = ((x + 3) % 4) * 2 + core
    far = ((x + 2) % 4) * 2 + core
    return me, x, core, x * 2 + 1 - core, right, left, far


def read_maps(pays, i):
    low = pays[i, 320:384, :].astype(F32)
    g1 = low[0:1, 64:65] + low[1:2, 64:65]
    g2 = low[2:3, 64:65] + low[3:4, 64:65]
    one = (pays[i, 0:128, :], pays[i, 128:256, :].astype(F32), g1)
    two = (pays[i, 320:384, :][:, :64], pays[i, 256:320, :].astype(F32), g2)
    return one, two


def after(earlier, later):
    d0, a0, g0 = earlier
    d1, a1, g1 = later
    made = mm(d1, jnp.concatenate([a0, d0], axis=1))
    return (
        d0 * g1 + d1.astype(F32) * g0 + made[:, BLK:],
        a0 * g1 + a1 + made[:, :BLK],
        g0 * g1,
    )


def write_maps(pays, i, one, two):
    (d1, a1, g1), (d2, a2, g2) = one, two
    row = lax.broadcasted_iota(jnp.int32, (64, 64), 0)
    hi1, hi2 = g1.astype(BF16).astype(F32), g2.astype(BF16).astype(F32)
    scal = jnp.where(row == 0, jnp.broadcast_to(hi1, (64, 64)), 0.0)
    scal = scal + jnp.where(row == 1, jnp.broadcast_to(g1 - hi1, (64, 64)), 0.0)
    scal = scal + jnp.where(row == 2, jnp.broadcast_to(hi2, (64, 64)), 0.0)
    scal = scal + jnp.where(row == 3, jnp.broadcast_to(g2 - hi2, (64, 64)), 0.0)
    pays[i, 0:128, :] = d1.astype(BF16)
    pays[i, 128:256, :] = a1.astype(BF16)
    pays[i, 256:320, :] = a2.astype(BF16)
    pays[i, 320:384, :] = jnp.concatenate([d2, scal], axis=1).astype(BF16)


def layer_kernel(
    q1_in, k1_in, q2_in, k2_in, vals_in, gates_in, upd, fade, boost, level, bias, norm_coef,
    emission, chan_coef, hidden_in, w_gate, w_up, w_down, taps,
    out,
    beta_s, cum_s, keep_s, qd1, qd2, loc1, loc2, add1, add2, vf, gf, r1, r2, o1, o2,
    pays, row_pays, heads, arrived, emit_w, skip, normed, wall, wdt, wd_own,
    q1, k1, q2, k2, vals, gates, hidden,
    feat, low, hid, acc, d2d_out, d2d_in, far_out, msg_r, msg_l, far_in, in_l, in_r,
    load_sem, send_sem, recv_sem, wsend, wrecv,
):
    me, x, core, mate, right, left, far = ring_places()
    z, y = lax.axis_index("sp_0"), lax.axis_index("sp_1")
    place = z * 4 + y
    after_z, after_y = ((place + 1) % 16) // 4, (place + 1) % 4
    prior_z, prior_y = ((place + 15) % 16) // 4, (place + 15) % 4
    to_mate, to_right, to_left = {"tp": mate}, {"tp": right}, {"tp": left}
    to_next = {"sp_0": after_z, "sp_1": after_y}
    to_prior = {"sp_0": prior_z, "sp_1": prior_y}

    home = pl.ds(pl.multiple_of(place * 128, 128), 128)
    loads = [
        pltpu.make_async_copy(w_gate, wall.at[home, 0:UNITS], load_sem.at[0]),
        pltpu.make_async_copy(w_up, wall.at[home, UNITS : 2 * UNITS], load_sem.at[1]),
        pltpu.make_async_copy(w_down, wd_own, load_sem.at[2]),
        pltpu.make_async_copy(emission, emit_w, load_sem.at[3]),
    ]
    for c in loads[:3]:
        c.start()
    given = (q1_in, k1_in, q2_in, k2_in, vals_in, gates_in, hidden_in)
    taken = (q1, k1, q2, k2, vals, gates, hidden)
    for i in range(7):
        loads.append(pltpu.make_async_copy(given[i], taken[i], load_sem.at[4 + i]))
        loads[-1].start()
    loads[3].start()

    step = 1 - 2 * core
    at = (y, z)
    names = ("sp_1", "sp_0")
    ahead = ((y + step + 4) % 4, (z + step + 4) % 4)
    behind = ((y - step + 4) % 4, (z - step + 4) % 4)
    across = ((y + 2) % 4, (z + 2) % 4)

    barrier = pltpu.get_barrier_semaphore()
    peers = [{"tp": (me + i) % 8} for i in range(1, 8)]
    peers += [{names[d]: n[d]} for d in range(2) for n in (ahead, behind)]
    peers += [to_next, to_prior]
    for peer in peers:
        pl.semaphore_signal(barrier, inc=1, device_id=peer, device_id_type=MESH)

    def ring_copy(sems, k, kind, ref_at, dim):
        src = ref_at(behind[dim] if kind == 2 else at[dim])
        goal = behind[dim] if kind == 1 else ahead[dim]
        return pltpu.make_async_remote_copy(
            src_ref=src, dst_ref=src, send_sem=sems[0].at[k], recv_sem=sems[1].at[k],
            device_id={names[dim]: goal}, device_id_type=MESH,
        )

    def weight_block(along_y, along_z, kind, chunk):
        first = (along_z * 4 + along_y) * 128 + 64 * kind
        if chunk == 1:
            return wdt.at[along_z * 4 + along_y, pl.ds(384 * kind, 384), :]
        return wall.at[pl.ds(pl.multiple_of(first, 64), 64), :]

    def first_ring(chunk, kind, what):
        def ref_at(i):
            return weight_block(i, z, 0, chunk) if kind == 0 else weight_block(y, i, 1, chunk)

        return ring_copy((wsend, wrecv), (chunk * 2 + kind) * 15 + what, what, ref_at, kind)

    def second_ring(chunk, kind, piece, what):
        other = (at[kind], behind[kind], ahead[kind], across[kind])[piece]

        def ref_at(i):
            if kind == 0:
                return weight_block(other, i, 0, chunk)
            return weight_block(i, other, 1, chunk)

        k = (chunk * 2 + kind) * 15 + 3 + piece * 3 + what
        return ring_copy((wsend, wrecv), k, what, ref_at, 1 - kind)

    pl.semaphore_wait(barrier, 13)
    for chunk in range(2):
        for c in (loads[:2], loads[2:3])[chunk]:
            c.wait()
        if chunk == 1:
            for i in range(6):
                piece = slice(i * BLK, (i + 1) * BLK)
                wdt[place, piece, :] = wd_own[:, piece].astype(F32).T.astype(BF16)
        for kind in range(2):
            first_ring(chunk, kind, 0).start()
            first_ring(chunk, kind, 1).start()

    for c in loads[4:]:
        c.wait()
    vf[...] = vals[...].astype(F32)
    gf[...] = gates[...].astype(F32)
    for h in range(2):
        beta, cum = gate_rows(upd[...].astype(F32)[h : h + 1], fade[h], boost[h], level[0, h], bias[0, h])
        beta_s[h * NBLK : (h + 1) * NBLK, :] = beta
        cum_s[h * NBLK : (h + 1) * NBLK, :] = cum

    def parts(it, carry):
        todo = [(h, 2 * it + j) for j in range(2) for h in range(2)]
        ins = []
        for h, n in todo:
            rows = pl.ds(pl.multiple_of(n * BLK, BLK), BLK)
            if h == 0:
                q, k = q1[rows, :].astype(F32), k1[rows, :].astype(F32)
            else:
                q, k = q2[:, rows].astype(F32).T, k2[:, rows].astype(F32).T
            ins.append(
                block_inputs(
                    q,
                    k,
                    vf[pl.ds(2 * n * BLK + h, BLK, 2), :],
                    cum_s[pl.ds(h * NBLK + n, 1), :],
                    beta_s[pl.ds(h * NBLK + n, 1), :],
                )
            )
        extra = inverses([i["lower"] for i in ins])
        for (h, n), i, e in zip(todo, ins, extra):
            dk = (128, 64)[h]
            solved = (i["right"] + mm(e, i["right"])).astype(BF16)
            made = mm(jnp.concatenate([i["intra"], i["tail"]], axis=0), solved)
            qd, loc, add = ((qd1, loc1, add1), (qd2, loc2, add2))[h]
            qd[n, :BLK, :] = (i["query"] - made[:BLK, BLK:]).astype(BF16)
            qd[n, BLK:, :] = (-made[BLK:, BLK:]).astype(BF16)
            loc[n] = made[:BLK, :BLK]
            add[n] = made[BLK:, :BLK]
            keep_s[pl.ds(h * NBLK + n, 1), :] = i["keep"]
        return carry

    lax.fori_loop(0, 3, parts, 0)
    for kind in range(2):
        first_ring(0, kind, 0).wait_recv()
        first_ring(0, kind, 2).start()
        second_ring(0, kind, 0, 0).start()
        second_ring(0, kind, 0, 1).start()
    lax.fori_loop(3, NBLK // 2, parts, 0)
    for kind in range(2):
        first_ring(1, kind, 0).wait_recv()
        first_ring(1, kind, 2).start()

    def eye(dk):
        return (
            lax.broadcasted_iota(jnp.int32, (dk, dk), 0)
            == lax.broadcasted_iota(jnp.int32, (dk, dk), 1)
        ).astype(F32)

    def chain(n, carry):
        rows = pl.ds(pl.multiple_of(n * BLK, BLK), BLK)
        out = []
        for h, (state, total) in enumerate(carry):
            dk = (128, 64)[h]
            qd, loc, add = ((qd1, loc1, add1), (qd2, loc2, add2))[h]
            r, o = ((r1, o1), (r2, o2))[h]
            made = mm(qd[n], state)
            o[rows, :] = loc[n] + made[:BLK, :BLK]
            r[rows, :] = made[:BLK, BLK:].astype(BF16)
            keep = keep_s[pl.ds(h * NBLK + n, 1), :]
            moved = made[BLK:]
            new_a = state[:, :BLK] * keep + moved[:, :BLK] + add[n]
            new_p = state[:, BLK:] * keep[:, :dk] + moved[:, BLK:]
            out.append((jnp.concatenate([new_a, new_p], axis=1), total * keep))
        return tuple(out)

    start = tuple(
        (jnp.concatenate([jnp.zeros((dk, BLK), F32), eye(dk)], axis=1), jnp.ones((1, BLK), F32))
        for dk in (128, 64)
    )
    (s1, g1), (s2, g2) = lax.fori_loop(0, NBLK, chain, start)
    write_maps(
        pays,
        y,
        (s1[:, BLK:] - eye(128) * g1, s1[:, :BLK], g1[:, :1]),
        (s2[:, BLK:] - eye(64) * g2[:, :64], s2[:, :BLK], g2[:, :1]),
    )

    def exchange(buf, dim, what):
        sems = (send_sem, recv_sem)
        return ring_copy(sems, 22 + dim * 3 + what, what, lambda i: buf.at[i], dim)

    exchange(pays, 0, 0).start()
    exchange(pays, 0, 1).start()
    first_ring(0, 0, 1).wait_recv()
    first_ring(0, 0, 2).wait_recv()
    for piece in (1,):
        second_ring(0, 0, piece, 0).start()
        second_ring(0, 0, piece, 1).start()
    exchange(pays, 0, 0).wait_recv()
    exchange(pays, 0, 2).start()
    for piece in (0,):
        second_ring(0, 0, piece, 0).wait_recv()
        second_ring(0, 0, piece, 2).start()
    for piece in (0,):
        second_ring(0, 1, piece, 0).wait_recv()
        second_ring(0, 1, piece, 2).start()
    exchange(pays, 0, 1).wait_recv()
    exchange(pays, 0, 2).wait_recv()
    whole = read_maps(pays, 0)
    whole = tuple((d.astype(F32), a, g) for d, a, g in whole)
    for i in range(1, 4):
        whole = tuple(after(e, l) for e, l in zip(whole, read_maps(pays, i)))
    write_maps(row_pays, z, *whole)
    exchange(row_pays, 1, 0).start()
    exchange(row_pays, 1, 1).start()
    first_ring(0, 1, 1).wait_recv()
    first_ring(0, 1, 2).wait_recv()
    for piece in (1, 2, 3):
        second_ring(0, 1, piece, 0).start()
        second_ring(0, 1, piece, 1).start()
    exchange(row_pays, 1, 0).wait_recv()
    exchange(row_pays, 1, 2).start()
    for piece in (2, 3):
        second_ring(0, 0, piece, 0).start()
        second_ring(0, 0, piece, 1).start()
    exchange(row_pays, 1, 1).wait_recv()
    exchange(row_pays, 1, 2).wait_recv()

    states = [jnp.zeros((128, BLK), F32), jnp.zeros((64, BLK), F32)]
    for buf, limit in ((row_pays, z), (pays, y)):
        for i in range(3):
            moved = [
                s * g + a + mm(d, s) for (d, a, g), s in zip(read_maps(buf, i), states)
            ]
            states = [jnp.where(i < limit, m, s) for m, s in zip(moved, states)]
    states = [s.astype(BF16) for s in states]

    order = (far, far + 1 - 2 * core, right, right + 1 - 2 * core, left, left + 1 - 2 * core, mate)

    def finish(n):
        rows = pl.ds(pl.multiple_of(n * BLK, BLK), BLK)
        for h in range(2):
            o, r = ((o1, r1), (o2, r2))[h]
            head = o[rows, :] + mm(r[rows, :], states[h])
            scale = lax.rsqrt(jnp.mean(head * head, axis=-1, keepdims=True) + EPSILON)
            g = gf[pl.ds(2 * n * BLK + h, BLK, 2), :]
            made = head * scale * norm_coef[...] * (0.5 * g * (1.0 + jnp.tanh(0.5 * g)))
            heads[n, :, h * BLK : (h + 1) * BLK] = made.astype(BF16)

    def hand_out(k):
        return pltpu.make_async_remote_copy(
            src_ref=heads.at[order[k]], dst_ref=arrived.at[me],
            send_sem=send_sem.at[28 + k], recv_sem=recv_sem.at[28 + k],
            device_id={"tp": order[k]}, device_id_type=MESH,
        )

    for piece in (1,):
        second_ring(0, 0, piece, 0).wait_recv()
        second_ring(0, 0, piece, 2).start()
    for k in range(7):
        finish(order[k])
        hand_out(k).start()
    finish(me)
    arrived[me] = heads[me]
    for piece in (1,):
        second_ring(0, 1, piece, 0).wait_recv()
        second_ring(0, 1, piece, 2).start()
    skip[...] = hidden[...].astype(F32)
    loads[3].wait()

    def emit(pair):
        firsts = [arrived[2 * pair + i] for i in range(2)]
        one = jnp.concatenate([f[:, :BLK] for f in firsts], axis=1)
        two = jnp.concatenate([f[:, BLK:] for f in firsts], axis=1)
        upper = pl.ds(pl.multiple_of(pair * 256, 256), 256)
        lower = pl.ds(pl.multiple_of(pair * 256 + 1024, 256), 256)

        def tile(j, carry):
            cols = pl.ds(pl.multiple_of(j * 512, 512), 512)
            skip[:, cols] += mm(one, emit_w[upper, cols]) + mm(two, emit_w[lower, cols])
            return carry

        lax.fori_loop(0, 4, tile, 0, unroll=2)

    hand_out(6).wait_recv()
    emit(x)
    for piece in (2,):
        second_ring(0, 1, piece, 0).wait_recv()
        second_ring(0, 1, piece, 2).start()
    for piece in (2,):
        second_ring(0, 0, piece, 0).wait_recv()
        second_ring(0, 0, piece, 2).start()
    hand_out(2).wait_recv()
    hand_out(3).wait_recv()
    emit((x + 3) % 4)
    for piece in (3,):
        second_ring(0, 1, piece, 0).wait_recv()
        second_ring(0, 1, piece, 2).start()
    for piece in (3,):
        second_ring(0, 0, piece, 0).wait_recv()
        second_ring(0, 0, piece, 2).start()
    hand_out(4).wait_recv()
    hand_out(5).wait_recv()
    emit((x + 1) % 4)
    first_ring(1, 0, 1).wait_recv()
    first_ring(1, 0, 2).wait_recv()
    first_ring(1, 1, 1).wait_recv()
    first_ring(1, 1, 2).wait_recv()
    for piece in range(4):
        second_ring(1, 0, piece, 0).start()
        second_ring(1, 0, piece, 1).start()
    for piece in range(4):
        second_ring(1, 1, piece, 0).start()
        second_ring(1, 1, piece, 1).start()
    hand_out(0).wait_recv()
    hand_out(1).wait_recv()
    emit((x + 2) % 4)
    full = skip[...]
    norm = lax.rsqrt(jnp.mean(full * full, axis=-1, keepdims=True) + EPSILON)
    normed[...] = (full * norm * chan_coef[...]).astype(BF16)

    def send(k, src, dst, peer):
        return pltpu.make_async_remote_copy(
            src_ref=src, dst_ref=dst, send_sem=send_sem.at[k], recv_sem=recv_sem.at[k],
            device_id=peer, device_id_type=MESH,
        )

    def shard(i, first=0, count=128):
        return feat.at[pl.ds(pl.multiple_of(i * 128 + first, 64), count), :]

    half_a, half_b = normed.at[0:64, :], normed.at[64:128, :]
    own_mate = send(0, normed, shard(me), to_mate)
    own = [
        send(1, half_a, shard(me, 0, 64), to_right),
        send(3, half_b, shard(me, 64, 64), to_left),
        send(2, half_b, shard(me, 64, 64), to_right),
        send(4, half_a, shard(me, 0, 64), to_left),
    ]
    own_mate.start()
    for c in own:
        c.start()
    a_right, b_left, b_right, a_left = tuple(own)
    fwd_a = send(5, shard(left, 0, 64), shard(left, 0, 64), to_right)
    fwd_b = send(6, shard(right, 64, 64), shard(right, 64, 64), to_left)
    mate_la = send(7, shard(left, 0, 64), shard(left, 0, 64), to_mate)
    mate_rb = send(8, shard(right, 64, 64), shard(right, 64, 64), to_mate)
    mate_lb = send(35, shard(left, 64, 64), shard(left, 64, 64), to_mate)
    mate_ra = send(36, shard(right, 0, 64), shard(right, 0, 64), to_mate)
    mate_fa = send(9, shard(far, 0, 64), shard(far, 0, 64), to_mate)
    mate_fb = send(10, shard(far, 64, 64), shard(far, 64, 64), to_mate)
    halo = send(11, low.at[:, 1024:1032, :], low.at[:, 0:8, :], to_next)

    feat[pl.ds(pl.multiple_of(me * 128, 128), 128), :] = normed[...]

    def gate_up(segments, first=0, last=6):
        count = 256 // len(segments)
        starts = [pl.multiple_of(s, 64) for s in segments]

        def tile(j, carry):
            cols = pl.ds(pl.multiple_of(j * 256, 256), 256)
            rows = jnp.concatenate([feat[pl.ds(s, count), :] for s in starts], axis=0)
            made = mm(rows, wall[:, cols]).astype(BF16).astype(F32)
            for i, s in enumerate(starts):
                for half in range(2):
                    low[2 * j + half, pl.ds(pl.multiple_of(s + 8, 8), count), :] = made[
                        i * count : (i + 1) * count, half * BLK : (half + 1) * BLK
                    ]
            return carry

        lax.fori_loop(first, last, tile, 0, unroll=2 if (last - first) % 2 == 0 else 3)

    def conv(pair, first, count):
        start = pair * 256 + first

        def mix(j, carry):
            span = pl.ds(pl.multiple_of(j * BLK, BLK), BLK)
            total = []
            for side in range(2):
                t = [taps[i, side : side + 1, span].astype(F32) for i in range(3)]
                w = [low[j + 6 * side, pl.ds(start + 6 + i, count), :] for i in range(3)]
                total.append(t[0] * w[0] + t[1] * w[1] + t[2] * w[2])
            g, u = total
            rows = pl.ds(pl.multiple_of(start, 64), count)
            hid[rows, span] = (0.5 * g * (1.0 + jnp.tanh(0.5 * g)) * u).astype(BF16)
            return carry

        lax.fori_loop(0, 6, mix, 0)

    wide = (slice(0, 1024), slice(1024, 2048))

    def down(k, pair, sem, first=0, count=128, part=None):
        mine = pl.ds(pl.multiple_of(pair * 256 + core * 128 + first, 64), count)
        other = pl.ds(pl.multiple_of(pair * 256 + (1 - core) * 128 + first, 64), count)
        kept = slice(first, first + count)

        def tile(j, carry):
            span = pl.ds(pl.multiple_of(j * 256, 256), 256)
            both = jnp.concatenate([hid[mine, :], hid[other, :]], axis=0)
            made = mm(both, jnp.concatenate([wdt[2 * j], wdt[2 * j + 1]], axis=1))
            acc[k, kept, span] = made[:count]
            d2d_out[k, kept, span] = made[count:].astype(BF16)
            return carry

        tiles, cols = ((0, 8), slice(None)) if part is None else ((4 * part, 4 * part + 4), wide[part])
        lax.fori_loop(*tiles, tile, 0, unroll=4)
        sent = send(sem, d2d_out.at[k, kept, cols], d2d_in.at[k, kept, cols], to_mate)
        sent.start()
        return sent

    def pair_sum(k, kept, cols=slice(None)):
        return acc[k, kept, cols] + d2d_in[k, kept, cols].astype(F32)

    top, bottom = slice(0, 64), slice(64, 128)
    pair_r, pair_l, pair_f = (x + 1) % 4, (x + 3) % 4, (x + 2) % 4
    far_b = [
        send((16, 38)[c], far_out.at[bottom, wide[c]], far_in.at[bottom, wide[c]], to_right)
        for c in range(2)
    ]
    far_a = [
        send((17, 39)[c], far_out.at[top, wide[c]], far_in.at[top, wide[c]], to_left)
        for c in range(2)
    ]
    r_a = [
        send((18, 45)[c], msg_r.at[top, wide[c]], in_l.at[top, wide[c]], to_right)
        for c in range(2)
    ]
    r_b = [
        send((19, 40)[c], msg_r.at[bottom, wide[c]], in_l.at[bottom, wide[c]], to_right)
        for c in range(2)
    ]
    l_b = [
        send((20, 46)[c], msg_l.at[bottom, wide[c]], in_r.at[bottom, wide[c]], to_left)
        for c in range(2)
    ]
    l_a = [
        send((21, 41)[c], msg_l.at[top, wide[c]], in_r.at[top, wide[c]], to_left)
        for c in range(2)
    ]

    for kind in range(2):
        second_ring(0, kind, 0, 1).wait_recv()
        second_ring(0, kind, 0, 2).wait_recv()
        for piece in (1, 2, 3):
            second_ring(0, kind, piece, 1).wait_recv()
            second_ring(0, kind, piece, 2).wait_recv()
    own_mate.wait_recv()
    gate_up([x * 256])

    @pl.when(x == 3)
    def _():
        halo.start()

    a_right.wait_recv()
    fwd_a.start()
    mate_la.start()
    b_left.wait_recv()
    fwd_b.start()
    mate_rb.start()
    mate_la.wait_recv()
    mate_rb.wait_recv()
    early = [pair_l * 256, pair_l * 256 + 128, pair_r * 256 + 64, pair_r * 256 + 192]
    for kind in range(2):
        for piece in range(4):
            second_ring(1, kind, piece, 0).wait_recv()
            second_ring(1, kind, piece, 2).start()
    gate_up(early, 0, 4)
    b_right.wait_recv()
    mate_lb.start()
    a_left.wait_recv()
    mate_ra.start()
    gate_up(early, 4, 6)
    mate_lb.wait_recv()
    mate_ra.wait_recv()
    gate_up([pair_l * 256 + 64, pair_l * 256 + 192, pair_r * 256, pair_r * 256 + 128])

    @pl.when(jnp.logical_or(x == 2, x == 0))
    def _():
        halo.start()

    @pl.when(x == 3)
    def _():
        halo.wait_recv()

    @pl.when(jnp.logical_and(place == 0, x == 3))
    def _():
        low[:, 0:8, :] = jnp.zeros((12, 8, BLK), F32)

    conv(pair_r, 0, 256)
    conv(pair_l, 64, 64)
    conv(pair_l, 192, 64)
    fwd_a.wait_recv()
    mate_fa.start()
    fwd_b.wait_recv()
    mate_fb.start()
    for kind in range(2):
        for piece in range(4):
            second_ring(1, kind, piece, 1).wait_recv()
            second_ring(1, kind, piece, 2).wait_recv()
    d_right, d_left_b = [], []
    for c in range(2):
        d_right.append(down(1, pair_r, (12, 43)[c], part=c))
        d_left_b.append(down(2, pair_l, (13, 44)[c], 64, 64, part=c))
    mate_fa.wait_recv()
    mate_fb.wait_recv()
    for c in range(2):
        gate_up([pair_f * 256], 2 * c, 2 * c + 2)
        d_right[c].wait_recv()
        msg_r[top, wide[c]] = pair_sum(1, top, wide[c]).astype(BF16)
        r_a[c].start()
        d_left_b[c].wait_recv()
        msg_l[bottom, wide[c]] = pair_sum(2, bottom, wide[c]).astype(BF16)
        l_b[c].start()
    gate_up([pair_f * 256], 4, 6)

    @pl.when(x == 1)
    def _():
        halo.start()

    @pl.when(x == 2)
    def _():
        halo.wait_recv()

    @pl.when(jnp.logical_and(place == 0, x == 2))
    def _():
        low[:, 0:8, :] = jnp.zeros((12, 8, BLK), F32)

    conv(pair_f, 0, 256)
    d_far = [down(0, pair_f, (14, 42)[c], part=c) for c in range(2)]
    for c in range(2):
        d_far[c].wait_recv()
        far_out[:, wide[c]] = pair_sum(0, slice(0, 128), wide[c]).astype(BF16)
        far_a[c].start()
        far_b[c].start()

    @pl.when(x < 2)
    def _():
        halo.wait_recv()

    @pl.when(jnp.logical_and(place == 0, x < 2))
    def _():
        low[:, 0:8, :] = jnp.zeros((12, 8, BLK), F32)

    conv(pair_l, 0, 64)
    conv(pair_l, 128, 64)
    d_left_a = down(2, pair_l, 37, 0, 64)
    conv(x, 0, 256)
    d_own = down(3, x, 15)
    d_left_a.wait_recv()
    acc[2, top, :] = pair_sum(2, top)
    acc[1, bottom, :] = pair_sum(1, bottom)
    for c in range(2):
        cols = wide[c]
        far_a[c].wait_recv()
        msg_l[top, cols] = (acc[2, top, cols] + far_in[top, cols].astype(F32)).astype(BF16)
        l_a[c].start()
        far_b[c].wait_recv()
        msg_r[bottom, cols] = (
            acc[1, bottom, cols] + far_in[bottom, cols].astype(F32)
        ).astype(BF16)
        r_b[c].start()
    d_own.wait_recv()
    acc[3] = acc[3] + d2d_in[3].astype(F32) + skip[...]
    for c in (*r_a, *l_b):
        c.wait_recv()
    acc[3, top, :] = acc[3, top, :] + in_l[top, :].astype(F32)
    acc[3, bottom, :] = acc[3, bottom, :] + in_r[bottom, :].astype(F32)
    for c in range(2):
        cols = wide[c]
        l_a[c].wait_recv()
        out[top, cols] = (acc[3, top, cols] + in_r[top, cols].astype(F32)).astype(BF16)
        r_b[c].wait_recv()
        out[bottom, cols] = (acc[3, bottom, cols] + in_l[bottom, cols].astype(F32)).astype(BF16)

    for c in (own_mate, *own, fwd_a, fwd_b, mate_la, mate_lb, mate_ra, mate_rb, mate_fa, mate_fb):
        c.wait_send()
    for c in (halo, *d_far, *d_right, d_left_a, *d_left_b, d_own, *far_a, *far_b):
        c.wait_send()
    for c in (*r_a, *r_b, *l_a, *l_b):
        c.wait_send()
    for dim, buf in ((0, pays), (1, row_pays)):
        for what in range(3):
            exchange(buf, dim, what).wait_send()
    for k in range(7):
        hand_out(k).wait_send()
    for chunk in range(2):
        for kind in range(2):
            for what in range(3):
                first_ring(chunk, kind, what).wait_send()
                for piece in range(4):
                    second_ring(chunk, kind, piece, what).wait_send()


def whole_layer(*args):
    vm = pl.BlockSpec(memory_space=pltpu.VMEM)
    sm = pl.BlockSpec(memory_space=pltpu.SMEM)
    hbm = pl.BlockSpec(memory_space=pl.ANY)
    block = [(128, WIDTH)] * 6
    return pl.pallas_call(
        layer_kernel,
        out_shape=jax.ShapeDtypeStruct((128, WIDTH), BF16),
        in_specs=[hbm] * 6 + [vm] * 3 + [sm] * 2 + [vm, hbm, vm, hbm, hbm, hbm, hbm, vm],
        out_specs=vm,
        scratch_shapes=[
            *[pltpu.VMEM((2 * NBLK, BLK), F32)] * 3,
            pltpu.VMEM((NBLK, 256, 128), BF16),
            pltpu.VMEM((NBLK, 192, 64), BF16),
            pltpu.VMEM((NBLK, BLK, BLK), F32),
            pltpu.VMEM((NBLK, BLK, BLK), F32),
            pltpu.VMEM((NBLK, 128, BLK), F32),
            pltpu.VMEM((NBLK, 64, BLK), F32),
            pltpu.VMEM((2048, BLK), F32),
            pltpu.VMEM((2048, BLK), F32),
            pltpu.VMEM((1024, 128), BF16),
            pltpu.VMEM((1024, 64), BF16),
            pltpu.VMEM((1024, BLK), F32),
            pltpu.VMEM((1024, BLK), F32),
            pltpu.VMEM((4, 384, 128), BF16),
            pltpu.VMEM((4, 384, 128), BF16),
            pltpu.VMEM((8, 128, 256), BF16),
            pltpu.VMEM((8, 128, 256), BF16),
            pltpu.VMEM((WIDTH, WIDTH), BF16),
            pltpu.VMEM((128, WIDTH), F32),
            pltpu.VMEM((128, WIDTH), BF16),
            pltpu.VMEM((WIDTH, 2 * UNITS), BF16),
            pltpu.VMEM((16, UNITS, BLK), BF16),
            pltpu.VMEM((128, UNITS), BF16),
            *[pltpu.VMEM((1024, 128), BF16)] * 2,
            *[pltpu.VMEM((64, 1024), BF16)] * 2,
            *[pltpu.VMEM((2048, BLK), BF16)] * 2,
            pltpu.VMEM((128, WIDTH), BF16),
            pltpu.VMEM((1024, WIDTH), BF16),
            pltpu.VMEM((12, 1032, BLK), F32),
            pltpu.VMEM((1024, UNITS), BF16),
            pltpu.VMEM((4, 128, WIDTH), F32),
            pltpu.VMEM((4, 128, WIDTH), BF16),
            pltpu.VMEM((4, 128, WIDTH), BF16),
            *[pltpu.VMEM(b, BF16) for b in block],
            pltpu.SemaphoreType.DMA((11,)),
            pltpu.SemaphoreType.DMA((47,)),
            pltpu.SemaphoreType.DMA((47,)),
            pltpu.SemaphoreType.DMA((60,)),
            pltpu.SemaphoreType.DMA((60,)),
        ],
        compiler_params=pltpu.CompilerParams(
            collective_id=1, has_side_effects=True, vmem_limit_bytes=62 * 1024 * 1024
        ),
    )(*args)


def per_device(
    arriving_hidden_state,
    former_request_vectors,
    former_match_vectors,
    latter_request_vectors,
    latter_match_vectors,
    stored_vectors_both,
    closing_valve_operands,
    update_level_before_squash,
    fading_data_input,
    sparse_fading_boost,
    unitwise_fading_loglevel,
    fading_constant_term,
    unitwise_normalizer_coef,
    emission_map_weights,
    channel_normalizer_coef,
    switching_channel_map,
    broadening_channel_map,
    timewise_convolve_tapvalues,
    narrowing_map_weights_in,
):
    return whole_layer(
        former_request_vectors,
        former_match_vectors,
        latter_request_vectors.T,
        latter_match_vectors.T,
        stored_vectors_both.reshape(-1, 128),
        closing_valve_operands.reshape(-1, 128),
        update_level_before_squash.reshape(2, -1),
        fading_data_input,
        sparse_fading_boost,
        unitwise_fading_loglevel.reshape(1, 2),
        fading_constant_term.reshape(1, 2),
        unitwise_normalizer_coef.reshape(1, -1),
        emission_map_weights,
        channel_normalizer_coef.reshape(1, -1),
        arriving_hidden_state,
        switching_channel_map,
        broadening_channel_map,
        narrowing_map_weights_in,
        timewise_convolve_tapvalues,
    )


def solution(mesh):
    torus = Mesh(mesh.devices.reshape(4, 4, mesh.shape["tp"]), ("sp_0", "sp_1", "tp"))
    return jax.shard_map(
        per_device,
        mesh=torus,
        in_specs=(
            P(SP_TP, None),
            P(SP, "tp"),
            P(SP, "tp"),
            P(SP, "tp"),
            P(SP, "tp"),
            P(SP, None, "tp"),
            P(SP, None, "tp"),
            P(None, "tp", SP),
            P(None, "tp", SP),
            P(None, "tp", SP),
            P(None, "tp"),
            P(None, "tp"),
            P(),
            P(),
            P(),
            P(SP, "tp"),
            P(SP, "tp"),
            P(None, None, "tp"),
            P(SP, "tp"),
        ),
        out_specs=P(SP_TP, None),
        check_vma=False,
    )
```

```python
import jax
import jax.numpy as jnp
from jax import lax
from jax.experimental import pallas as pl
from jax.experimental.pallas import tpu as pltpu
from jax.sharding import Mesh
from jax.sharding import PartitionSpec as P

SP = ("sp_0", "sp_1")
SP_TP = ("sp_0", "sp_1", "tp")
MESH = pl.DeviceIdType.MESH
WIDTH = 2048
UNITS = 768

BLK = 128
NBLK = 8
EPSILON = 1e-06
F32 = jnp.float32
BF16 = jnp.bfloat16


def mm(a, b):
    return jnp.dot(a.astype(BF16), b.astype(BF16), preferred_element_type=F32)


def mm_nt(a, b):
    return lax.dot_general(
        a.astype(BF16), b.astype(BF16), (((1,), (1,)), ((), ())), preferred_element_type=F32
    )


def normed_rows(x, scale):
    return x * (lax.rsqrt(jnp.sum(x * x, axis=-1, keepdims=True) + EPSILON) * scale)


def fold_blocks(row):
    return jnp.concatenate([row[:, i * BLK : (i + 1) * BLK] for i in range(NBLK)], axis=0)


def gate_rows(upd, fade, boost, loglevel, bias):
    beta = 1.0 / (1.0 + jnp.exp(-fold_blocks(upd.astype(F32))))
    pre = fold_blocks(fade) + bias
    soft = jnp.maximum(pre, 0.0) + jnp.log1p(jnp.exp(-jnp.abs(pre)))
    rate = jnp.exp(jnp.full((NBLK, BLK), loglevel, F32))
    cum = fold_blocks(boost) - rate * soft
    lane = lax.broadcasted_iota(jnp.int32, (NBLK, BLK), 1)
    step = 1
    while step < BLK:
        cum = cum + jnp.where(lane >= step, pltpu.roll(cum, step, 1), 0.0)
        step *= 2
    return beta, cum


def block_inputs(q, k, v, cum_row, beta_row):
    dk = q.shape[-1]
    c_j = jnp.broadcast_to(cum_row, (BLK, BLK))
    c_i = c_j.T
    b_i = jnp.broadcast_to(beta_row, (BLK, BLK)).T
    row = lax.broadcasted_iota(jnp.int32, (BLK, BLK), 0)
    col = lax.broadcasted_iota(jnp.int32, (BLK, BLK), 1)
    decay = jnp.exp(jnp.where(row >= col, c_i - c_j, -1e30))
    e_i = jnp.exp(c_i)
    c_last = jnp.broadcast_to(cum_row[:, BLK - 1 :], (1, BLK))
    qn = normed_rows(q.astype(F32), dk**-0.5)
    kn = normed_rows(k.astype(F32), 1.0)
    kb = kn.astype(BF16)
    both = mm_nt(jnp.concatenate([kb, qn.astype(BF16)], axis=0), kb)
    lower = jnp.where(row > col, -(b_i * both[:BLK] * decay), 0.0)
    intra = (both[BLK:] * decay).astype(BF16)
    right = jnp.concatenate([v.astype(F32) * b_i, kn * (b_i * e_i)[:, :dk]], axis=1)
    tail = kn * jnp.exp(c_last - c_i)[:, :dk]
    return dict(
        lower=lower,
        intra=intra,
        right=right,
        tail=tail.T.astype(BF16),
        query=qn * e_i[:, :dk],
        keep=jnp.exp(c_last),
    )


def inverses(lowers):
    powers = [n.astype(BF16) for n in lowers]
    extra = list(lowers)
    power = [mm(p, p) for p in powers]
    for level in range(1, 7):
        pb = [p.astype(BF16) for p in power]
        if level < 6:
            wide = [
                mm(p, jnp.concatenate([e.astype(BF16), p], axis=1)) for p, e in zip(pb, extra)
            ]
            extra = [e + p + w[:, :BLK] for e, p, w in zip(extra, power, wide)]
            power = [w[:, BLK:] for w in wide]
        else:
            extra = [e + p + mm(q, e) for e, p, q in zip(extra, power, pb)]
    return extra


def ring_places():
    me = lax.axis_index("tp")
    x, core = me // 2, me % 2
    right = ((x + 1) % 4) * 2 + core
    left = ((x + 3) % 4) * 2 + core
    far = ((x + 2) % 4) * 2 + core
    return me, x, core, x * 2 + 1 - core, right, left, far


def after(earlier, later):
    d0, a0, g0 = earlier
    d1, a1, g1 = later
    made = mm(d1, jnp.concatenate([a0, d0], axis=1))
    return (
        d0 * g1 + d1.astype(F32) * g0 + made[:, BLK:],
        a0 * g1 + a1 + made[:, :BLK],
        g0 * g1,
    )


def read_map(h, buf, i):
    if h == 0:
        g = buf[i, 256:272, :].astype(F32)
        return buf[i, 0:128, :], buf[i, 128:256, :].astype(F32), g[0:1, 0:1] + g[1:2, 0:1]
    both = buf[i, 64:128, :]
    g = both.astype(F32)
    return both[:, :64], buf[i, 0:64, :].astype(F32), g[0:1, 64:65] + g[1:2, 64:65]


def write_map(h, buf, i, whole):
    d, a, g = whole
    shape = ((16, 128), (64, 64))[h]
    row = lax.broadcasted_iota(jnp.int32, shape, 0)
    high = g.astype(BF16).astype(F32)
    scal = jnp.where(row == 0, jnp.broadcast_to(high, shape), 0.0)
    scal = scal + jnp.where(row == 1, jnp.broadcast_to(g - high, shape), 0.0)
    if h == 0:
        buf[i, 0:128, :] = d.astype(BF16)
        buf[i, 128:256, :] = a.astype(BF16)
        buf[i, 256:272, :] = scal.astype(BF16)
    else:
        buf[i, 0:64, :] = a.astype(BF16)
        buf[i, 64:128, :] = jnp.concatenate([d, scal], axis=1).astype(BF16)


def layer_kernel(
    q1_in, k1_in, q2_in, k2_in, vals_in, gates_in, upd, fade, boost, level, bias, norm_coef,
    emission, chan_coef, hidden_in, w_gate, w_up, w_down, taps,
    out,
    beta_s, cum_s, keep_s, qd1, qd2, loc1, loc2, add1, add2, vf, gf, r1, r2, o1, o2,
    pay_a, pay_b, row_a, row_b, heads, arrived, emit_w, skip, normed, wall, wdt, wd_own,
    q1, k1, q2, k2, vals, gates, hidden,
    feat, low, hid, acc, d2d_out, d2d_in, far_out, msg_r, msg_l, far_in, in_l, in_r,
    load_sem, send_sem, recv_sem, wsend, wrecv,
):
    me, x, core, mate, right, left, far = ring_places()
    z, y = lax.axis_index("sp_0"), lax.axis_index("sp_1")
    place = z * 4 + y
    after_z, after_y = ((place + 1) % 16) // 4, (place + 1) % 4
    prior_z, prior_y = ((place + 15) % 16) // 4, (place + 15) % 4
    to_mate, to_right, to_left = {"tp": mate}, {"tp": right}, {"tp": left}
    to_next = {"sp_0": after_z, "sp_1": after_y}
    to_prior = {"sp_0": prior_z, "sp_1": prior_y}

    home = pl.ds(pl.multiple_of(place * 128, 128), 128)
    loads = [
        pltpu.make_async_copy(w_gate, wall.at[home, 0:UNITS], load_sem.at[0]),
        pltpu.make_async_copy(w_up, wall.at[home, UNITS : 2 * UNITS], load_sem.at[1]),
        pltpu.make_async_copy(w_down, wd_own, load_sem.at[2]),
        pltpu.make_async_copy(emission, emit_w, load_sem.at[3]),
    ]
    for c in loads[:3]:
        c.start()
    given = (q1_in, k1_in, q2_in, k2_in, vals_in, gates_in, hidden_in)
    taken = (q1, k1, q2, k2, vals, gates, hidden)
    for i in range(7):
        loads.append(pltpu.make_async_copy(given[i], taken[i], load_sem.at[4 + i]))
        loads[-1].start()
    loads[3].start()

    step = 1 - 2 * core
    at = (y, z)
    names = ("sp_1", "sp_0")
    ahead = ((y + step + 4) % 4, (z + step + 4) % 4)
    behind = ((y - step + 4) % 4, (z - step + 4) % 4)
    across = ((y + 2) % 4, (z + 2) % 4)

    barrier = pltpu.get_barrier_semaphore()
    peers = [{"tp": (me + i) % 8} for i in range(1, 8)]
    peers += [{names[d]: n[d]} for d in range(2) for n in (ahead, behind)]
    peers += [to_next, to_prior]
    for peer in peers:
        pl.semaphore_signal(barrier, inc=1, device_id=peer, device_id_type=MESH)

    def ring_copy(sems, k, kind, ref_at, dim):
        src = ref_at(behind[dim] if kind == 2 else at[dim])
        goal = behind[dim] if kind == 1 else ahead[dim]
        return pltpu.make_async_remote_copy(
            src_ref=src, dst_ref=src, send_sem=sems[0].at[k], recv_sem=sems[1].at[k],
            device_id={names[dim]: goal}, device_id_type=MESH,
        )

    def weight_block(along_y, along_z, kind, chunk):
        first = (along_z * 4 + along_y) * 128 + 64 * kind
        if chunk == 1:
            return wdt.at[along_z * 4 + along_y, pl.ds(384 * kind, 384), :]
        return wall.at[pl.ds(pl.multiple_of(first, 64), 64), :]

    def first_ring(chunk, kind, what):
        def ref_at(i):
            return weight_block(i, z, 0, chunk) if kind == 0 else weight_block(y, i, 1, chunk)

        return ring_copy((wsend, wrecv), (chunk * 2 + kind) * 15 + what, what, ref_at, kind)

    def second_ring(chunk, kind, piece, what):
        other = (at[kind], behind[kind], ahead[kind], across[kind])[piece]

        def ref_at(i):
            if kind == 0:
                return weight_block(other, i, 0, chunk)
            return weight_block(i, other, 1, chunk)

        k = (chunk * 2 + kind) * 15 + 3 + piece * 3 + what
        return ring_copy((wsend, wrecv), k, what, ref_at, 1 - kind)

    pl.semaphore_wait(barrier, 13)
    for chunk in range(2):
        for c in (loads[:2], loads[2:3])[chunk]:
            c.wait()
        if chunk == 1:
            for i in range(6):
                piece = slice(i * BLK, (i + 1) * BLK)
                wdt[place, piece, :] = wd_own[:, piece].astype(F32).T.astype(BF16)
        for kind in range(2):
            first_ring(chunk, kind, 0).start()
            first_ring(chunk, kind, 1).start()

    for c in loads[4:]:
        c.wait()
    pays, row_pays = (pay_a, pay_b), (row_a, row_b)
    vf[...] = vals[...].astype(F32)
    gf[...] = gates[...].astype(F32)
    for h in range(2):
        beta, cum = gate_rows(
            upd[...].astype(F32)[h : h + 1], fade[h], boost[h], level[0, h], bias[0, h]
        )
        beta_s[h * NBLK : (h + 1) * NBLK, :] = beta
        cum_s[h * NBLK : (h + 1) * NBLK, :] = cum

    kept = ((qd1, loc1, add1, r1, o1), (qd2, loc2, add2, r2, o2))
    sizes = (128, 64)

    def parts_of(h):
        qd, loc, add = kept[h][:3]

        def parts(it, carry):
            todo = [4 * it + j for j in range(4)]
            ins = []
            for n in todo:
                rows = pl.ds(pl.multiple_of(n * BLK, BLK), BLK)
                if h == 0:
                    q, k = q1[rows, :].astype(F32), k1[rows, :].astype(F32)
                else:
                    q, k = q2[:, rows].astype(F32).T, k2[:, rows].astype(F32).T
                ins.append(
                    block_inputs(
                        q,
                        k,
                        vf[pl.ds(2 * n * BLK + h, BLK, 2), :],
                        cum_s[pl.ds(h * NBLK + n, 1), :],
                        beta_s[pl.ds(h * NBLK + n, 1), :],
                    )
                )
            extra = inverses([i["lower"] for i in ins])
            for n, i, e in zip(todo, ins, extra):
                solved = (i["right"] + mm(e, i["right"])).astype(BF16)
                made = mm(jnp.concatenate([i["intra"], i["tail"]], axis=0), solved)
                qd[n, :BLK, :] = (i["query"] - made[:BLK, BLK:]).astype(BF16)
                qd[n, BLK:, :] = (-made[BLK:, BLK:]).astype(BF16)
                loc[n] = made[:BLK, :BLK]
                add[n] = made[BLK:, :BLK]
                keep_s[pl.ds(h * NBLK + n, 1), :] = i["keep"]
            return carry

        return parts

    def eye(dk):
        return (
            lax.broadcasted_iota(jnp.int32, (dk, dk), 0)
            == lax.broadcasted_iota(jnp.int32, (dk, dk), 1)
        ).astype(F32)

    def local_map(h):
        dk = sizes[h]
        qd, loc, add, r, o = kept[h]

        def chain(n, carry):
            state, total = carry
            rows = pl.ds(pl.multiple_of(n * BLK, BLK), BLK)
            made = mm(qd[n], state)
            o[rows, :] = loc[n] + made[:BLK, :BLK]
            r[rows, :] = made[:BLK, BLK:].astype(BF16)
            keep = keep_s[pl.ds(h * NBLK + n, 1), :]
            moved = made[BLK:]
            new_a = state[:, :BLK] * keep + moved[:, :BLK] + add[n]
            new_p = state[:, BLK:] * keep[:, :dk] + moved[:, BLK:]
            return jnp.concatenate([new_a, new_p], axis=1), total * keep

        start = jnp.concatenate([jnp.zeros((dk, BLK), F32), eye(dk)], axis=1)
        state, total = lax.fori_loop(0, NBLK, chain, (start, jnp.ones((1, BLK), F32)))
        whole = (state[:, BLK:] - eye(dk) * total[:, :dk], state[:, :BLK], total[:, :1])
        write_map(h, pays[h], y, whole)

    def exchange(h, dim, what):
        buf = (pays, row_pays)[dim][h]
        k = 22 + (h * 2 + dim) * 3 + what
        return ring_copy((send_sem, recv_sem), k, what, lambda i: buf.at[i], dim)

    def first_wait(chunk, kind):
        first_ring(chunk, kind, 1).wait_recv()
        first_ring(chunk, kind, 2).wait_recv()

    def second_start(chunk, kind, pieces):
        for piece in pieces:
            second_ring(chunk, kind, piece, 0).start()
            second_ring(chunk, kind, piece, 1).start()

    def second_pass(chunk, kind, pieces):
        for piece in pieces:
            second_ring(chunk, kind, piece, 0).wait_recv()
            second_ring(chunk, kind, piece, 2).start()

    def row_total(h):
        exchange(h, 0, 1).wait_recv()
        exchange(h, 0, 2).wait_recv()
        d, a, g = read_map(h, pays[h], 0)
        whole = (d.astype(F32), a, g)
        for i in range(1, 4):
            whole = after(whole, read_map(h, pays[h], i))
        write_map(h, row_pays[h], z, whole)
        exchange(h, 1, 0).start()
        exchange(h, 1, 1).start()

    def incoming(h):
        exchange(h, 1, 1).wait_recv()
        exchange(h, 1, 2).wait_recv()
        state = jnp.zeros((sizes[h], BLK), F32)
        for buf, limit in ((row_pays[h], z), (pays[h], y)):
            for i in range(3):
                d, a, g = read_map(h, buf, i)
                state = jnp.where(i < limit, state * g + a + mm(d, state), state)
        return state.astype(BF16)

    order = (far, far + 1 - 2 * core, right, right + 1 - 2 * core, left, left + 1 - 2 * core, mate)

    def finish(h, n, state):
        r, o = kept[h][3:]
        rows = pl.ds(pl.multiple_of(n * BLK, BLK), BLK)
        head = o[rows, :] + mm(r[rows, :], state)
        scale = lax.rsqrt(jnp.mean(head * head, axis=-1, keepdims=True) + EPSILON)
        g = gf[pl.ds(2 * n * BLK + h, BLK, 2), :]
        made = head * scale * norm_coef[...] * (0.5 * g * (1.0 + jnp.tanh(0.5 * g)))
        heads[h, n] = made.astype(BF16)

    def hand_out(h, k):
        return pltpu.make_async_remote_copy(
            src_ref=heads.at[h, order[k]], dst_ref=arrived.at[h, me],
            send_sem=send_sem.at[47 + h * 7 + k], recv_sem=recv_sem.at[47 + h * 7 + k],
            device_id={"tp": order[k]}, device_id_type=MESH,
        )

    def finish_all(h, state):
        for k in range(7):
            finish(h, order[k], state)
            hand_out(h, k).start()
        finish(h, me, state)
        arrived[h, me] = heads[h, me]

    def emit(h, pair):
        rows = jnp.concatenate([arrived[h, 2 * pair + i] for i in range(2)], axis=1)
        span = pl.ds(pl.multiple_of(pair * 256 + h * 1024, 256), 256)

        def tile(j, carry):
            cols = pl.ds(pl.multiple_of(j * 512, 512), 512)
            skip[:, cols] += mm(rows, emit_w[span, cols])
            return carry

        lax.fori_loop(0, 4, tile, 0, unroll=2)

    lax.fori_loop(0, 2, parts_of(0), 0)
    local_map(0)
    exchange(0, 0, 0).start()
    exchange(0, 0, 1).start()
    for kind in range(2):
        first_ring(0, kind, 0).wait_recv()
        first_ring(0, kind, 2).start()
    second_start(0, 0, (0,))
    lax.fori_loop(0, 2, parts_of(1), 0)
    exchange(0, 0, 0).wait_recv()
    exchange(0, 0, 2).start()
    for kind in range(2):
        first_ring(1, kind, 0).wait_recv()
        first_ring(1, kind, 2).start()
    local_map(1)
    exchange(1, 0, 0).start()
    exchange(1, 0, 1).start()
    second_start(0, 1, (0,))
    row_total(0)
    first_wait(0, 0)
    second_ring(0, 0, 1, 0).start()
    exchange(1, 0, 0).wait_recv()
    exchange(1, 0, 2).start()
    first_wait(0, 1)
    second_start(0, 1, (1, 2, 3))
    exchange(0, 1, 0).wait_recv()
    exchange(0, 1, 2).start()
    row_total(1)
    second_ring(0, 0, 1, 1).start()
    state_a = incoming(0)
    exchange(1, 1, 0).wait_recv()
    exchange(1, 1, 2).start()
    second_pass(0, 0, (0,))
    second_start(0, 0, (2, 3))
    second_pass(0, 1, (0,))
    finish_all(0, state_a)
    second_pass(0, 0, (1,))
    state_b = incoming(1)
    finish_all(1, state_b)
    second_pass(0, 1, (1,))
    skip[...] = hidden[...].astype(F32)
    loads[3].wait()
    hand_out(0, 6).wait_recv()
    emit(0, x)
    for h in range(2):
        if h == 1:
            hand_out(1, 6).wait_recv()
            emit(1, x)
        hand_out(h, 2).wait_recv()
        hand_out(h, 3).wait_recv()
        emit(h, (x + 3) % 4)
        if h == 0:
            second_pass(0, 1, (2,))
        hand_out(h, 4).wait_recv()
        hand_out(h, 5).wait_recv()
        emit(h, (x + 1) % 4)
        second_pass(0, h, (2 + h,))
        hand_out(h, 0).wait_recv()
        hand_out(h, 1).wait_recv()
        emit(h, (x + 2) % 4)
    full = skip[...]
    norm = lax.rsqrt(jnp.mean(full * full, axis=-1, keepdims=True) + EPSILON)
    normed[...] = (full * norm * chan_coef[...]).astype(BF16)

    def send(k, src, dst, peer):
        return pltpu.make_async_remote_copy(
            src_ref=src, dst_ref=dst, send_sem=send_sem.at[k], recv_sem=recv_sem.at[k],
            device_id=peer, device_id_type=MESH,
        )

    def shard(i, first=0, count=128):
        return feat.at[pl.ds(pl.multiple_of(i * 128 + first, 64), count), :]

    half_a, half_b = normed.at[0:64, :], normed.at[64:128, :]
    own_mate = send(0, normed, shard(me), to_mate)
    own = [
        send(1, half_a, shard(me, 0, 64), to_right),
        send(3, half_b, shard(me, 64, 64), to_left),
        send(2, half_b, shard(me, 64, 64), to_right),
        send(4, half_a, shard(me, 0, 64), to_left),
    ]
    own_mate.start()
    for c in own:
        c.start()
    a_right, b_left, b_right, a_left = tuple(own)
    second_pass(0, 0, (3,))
    for kind in range(2):
        first_wait(1, kind)
    second_start(1, 1, range(4))
    second_start(1, 0, range(2))
    fwd_a = send(5, shard(left, 0, 64), shard(left, 0, 64), to_right)
    fwd_b = send(6, shard(right, 64, 64), shard(right, 64, 64), to_left)
    mate_la = send(7, shard(left, 0, 64), shard(left, 0, 64), to_mate)
    mate_rb = send(8, shard(right, 64, 64), shard(right, 64, 64), to_mate)
    mate_lb = send(35, shard(left, 64, 64), shard(left, 64, 64), to_mate)
    mate_ra = send(36, shard(right, 0, 64), shard(right, 0, 64), to_mate)
    mate_fa = send(9, shard(far, 0, 64), shard(far, 0, 64), to_mate)
    mate_fb = send(10, shard(far, 64, 64), shard(far, 64, 64), to_mate)
    halo = send(11, low.at[:, 1024:1032, :], low.at[:, 0:8, :], to_next)

    feat[pl.ds(pl.multiple_of(me * 128, 128), 128), :] = normed[...]

    def gate_up(segments, first=0, last=6):
        count = 256 // len(segments)
        starts = [pl.multiple_of(s, 64) for s in segments]

        def tile(j, carry):
            cols = pl.ds(pl.multiple_of(j * 256, 256), 256)
            rows = jnp.concatenate([feat[pl.ds(s, count), :] for s in starts], axis=0)
            made = mm(rows, wall[:, cols]).astype(BF16).astype(F32)
            for i, s in enumerate(starts):
                for half in range(2):
                    low[2 * j + half, pl.ds(pl.multiple_of(s + 8, 8), count), :] = made[
                        i * count : (i + 1) * count, half * BLK : (half + 1) * BLK
                    ]
            return carry

        lax.fori_loop(first, last, tile, 0, unroll=2 if (last - first) % 2 == 0 else 3)

    def conv(pair, first, count):
        start = pair * 256 + first

        def mix(j, carry):
            span = pl.ds(pl.multiple_of(j * BLK, BLK), BLK)
            total = []
            for side in range(2):
                t = [taps[i, side : side + 1, span].astype(F32) for i in range(3)]
                w = [low[j + 6 * side, pl.ds(start + 6 + i, count), :] for i in range(3)]
                total.append(t[0] * w[0] + t[1] * w[1] + t[2] * w[2])
            g, u = total
            rows = pl.ds(pl.multiple_of(start, 64), count)
            hid[rows, span] = (0.5 * g * (1.0 + jnp.tanh(0.5 * g)) * u).astype(BF16)
            return carry

        lax.fori_loop(0, 6, mix, 0)

    wide = (slice(0, 1024), slice(1024, 2048))

    offsets = [(a, b) for a in (0, 1, 3) for b in (0, 1, 3)]
    offsets += [(a, b) for a in range(4) for b in range(4) if a == 2 or b == 2]
    columns = [((z + a) % 4) * 4 + (y + b) % 4 for a, b in offsets]

    def down(k, pair, sem, first=0, count=128, part=None):
        mine = pl.ds(pl.multiple_of(pair * 256 + core * 128 + first, 64), count)
        other = pl.ds(pl.multiple_of(pair * 256 + (1 - core) * 128 + first, 64), count)
        kept = slice(first, first + count)

        tiles, cols = (range(8), slice(None))
        if part is not None:
            tiles, cols = (range(4 * part, 4 * part + 4), wide[part])
        both = jnp.concatenate([hid[mine, :], hid[other, :]], axis=0)
        for j in tiles:
            span = slice(256 * j, 256 * j + 256)
            weights = [wdt[columns[2 * j + i]] for i in range(2)]
            made = mm(both, jnp.concatenate(weights, axis=1))
            acc[k, kept, span] = made[:count]
            d2d_out[k, kept, span] = made[count:].astype(BF16)
        sent = send(sem, d2d_out.at[k, kept, cols], d2d_in.at[k, kept, cols], to_mate)
        sent.start()
        return sent

    def pair_sum(k, kept, cols=slice(None)):
        return acc[k, kept, cols] + d2d_in[k, kept, cols].astype(F32)

    top, bottom = slice(0, 64), slice(64, 128)
    pair_r, pair_l, pair_f = (x + 1) % 4, (x + 3) % 4, (x + 2) % 4
    far_b = [
        send((16, 38)[c], far_out.at[bottom, wide[c]], far_in.at[bottom, wide[c]], to_right)
        for c in range(2)
    ]
    far_a = [
        send((17, 39)[c], far_out.at[top, wide[c]], far_in.at[top, wide[c]], to_left)
        for c in range(2)
    ]
    r_a = [
        send((18, 45)[c], msg_r.at[top, wide[c]], in_l.at[top, wide[c]], to_right)
        for c in range(2)
    ]
    r_b = [
        send((19, 40)[c], msg_r.at[bottom, wide[c]], in_l.at[bottom, wide[c]], to_right)
        for c in range(2)
    ]
    l_b = [
        send((20, 46)[c], msg_l.at[bottom, wide[c]], in_r.at[bottom, wide[c]], to_left)
        for c in range(2)
    ]
    l_a = [
        send((21, 41)[c], msg_l.at[top, wide[c]], in_r.at[top, wide[c]], to_left)
        for c in range(2)
    ]

    for kind in range(2):
        second_ring(0, kind, 0, 1).wait_recv()
        second_ring(0, kind, 0, 2).wait_recv()
        for piece in (1, 2, 3):
            second_ring(0, kind, piece, 1).wait_recv()
            second_ring(0, kind, piece, 2).wait_recv()
    second_start(1, 0, (2, 3))
    own_mate.wait_recv()
    gate_up([x * 256])

    @pl.when(x == 3)
    def _():
        halo.start()

    a_right.wait_recv()
    fwd_a.start()
    mate_la.start()
    b_left.wait_recv()
    fwd_b.start()
    mate_rb.start()
    mate_la.wait_recv()
    mate_rb.wait_recv()
    early = [pair_l * 256, pair_l * 256 + 128, pair_r * 256 + 64, pair_r * 256 + 192]
    gate_up(early, 0, 4)
    for kind in range(2):
        for piece in range(4):
            second_ring(1, kind, piece, 0).wait_recv()
            second_ring(1, kind, piece, 2).start()
    b_right.wait_recv()
    mate_lb.start()
    a_left.wait_recv()
    mate_ra.start()
    gate_up(early, 4, 6)
    mate_lb.wait_recv()
    mate_ra.wait_recv()
    gate_up([pair_l * 256 + 64, pair_l * 256 + 192, pair_r * 256, pair_r * 256 + 128])

    @pl.when(jnp.logical_or(x == 2, x == 0))
    def _():
        halo.start()

    @pl.when(x == 3)
    def _():
        halo.wait_recv()

    @pl.when(jnp.logical_and(place == 0, x == 3))
    def _():
        low[:, 0:8, :] = jnp.zeros((12, 8, BLK), F32)

    conv(pair_r, 0, 256)
    conv(pair_l, 64, 64)
    conv(pair_l, 192, 64)
    for kind in range(2):
        for piece in range(4):
            second_ring(1, kind, piece, 1).wait_recv()
    d_right = [down(1, pair_r, 12, part=0)]
    d_left_b = [down(2, pair_l, 13, 64, 64, part=0)]
    fwd_a.wait_recv()
    mate_fa.start()
    fwd_b.wait_recv()
    mate_fb.start()

    def send_early(c):
        d_right[c].wait_recv()
        msg_r[top, wide[c]] = pair_sum(1, top, wide[c]).astype(BF16)
        r_a[c].start()
        d_left_b[c].wait_recv()
        msg_l[bottom, wide[c]] = pair_sum(2, bottom, wide[c]).astype(BF16)
        l_b[c].start()

    send_early(0)
    mate_fa.wait_recv()
    mate_fb.wait_recv()
    gate_up([pair_f * 256], 0, 4)
    for kind in range(2):
        for piece in range(4):
            second_ring(1, kind, piece, 2).wait_recv()
    d_right.append(down(1, pair_r, 43, part=1))
    d_left_b.append(down(2, pair_l, 44, 64, 64, part=1))
    gate_up([pair_f * 256], 4, 6)
    send_early(1)

    @pl.when(x == 1)
    def _():
        halo.start()

    @pl.when(x == 2)
    def _():
        halo.wait_recv()

    @pl.when(jnp.logical_and(place == 0, x == 2))
    def _():
        low[:, 0:8, :] = jnp.zeros((12, 8, BLK), F32)

    conv(pair_f, 0, 256)
    d_far = [down(0, pair_f, (14, 42)[c], part=c) for c in range(2)]
    for c in range(2):
        d_far[c].wait_recv()
        far_out[:, wide[c]] = pair_sum(0, slice(0, 128), wide[c]).astype(BF16)
        far_a[c].start()
        far_b[c].start()

    @pl.when(x < 2)
    def _():
        halo.wait_recv()

    @pl.when(jnp.logical_and(place == 0, x < 2))
    def _():
        low[:, 0:8, :] = jnp.zeros((12, 8, BLK), F32)

    conv(pair_l, 0, 64)
    conv(pair_l, 128, 64)
    d_left_a = down(2, pair_l, 37, 0, 64)
    conv(x, 0, 256)
    d_own = down(3, x, 15)
    d_left_a.wait_recv()
    acc[2, top, :] = pair_sum(2, top)
    acc[1, bottom, :] = pair_sum(1, bottom)
    for c in range(2):
        cols = wide[c]
        far_a[c].wait_recv()
        msg_l[top, cols] = (acc[2, top, cols] + far_in[top, cols].astype(F32)).astype(BF16)
        l_a[c].start()
        far_b[c].wait_recv()
        msg_r[bottom, cols] = (
            acc[1, bottom, cols] + far_in[bottom, cols].astype(F32)
        ).astype(BF16)
        r_b[c].start()
    d_own.wait_recv()
    acc[3] = acc[3] + d2d_in[3].astype(F32)
    for c in (*r_a, *l_b):
        c.wait_recv()
    acc[3, top, :] = acc[3, top, :] + in_l[top, :].astype(F32)
    acc[3, bottom, :] = acc[3, bottom, :] + in_r[bottom, :].astype(F32)
    for c in range(2):
        for rows, last, came in ((top, l_a, in_r), (bottom, r_b, in_l)):
            last[c].wait_recv()
            for i in range(8 * c, 8 * c + 8):
                slot = slice(i * BLK, (i + 1) * BLK)
                place_cols = pl.ds(pl.multiple_of(columns[i] * BLK, BLK), BLK)
                total = acc[3, rows, slot] + came[rows, slot].astype(F32)
                out[rows, place_cols] = (total + skip[rows, place_cols]).astype(BF16)

    for c in (own_mate, *own, fwd_a, fwd_b, mate_la, mate_lb, mate_ra, mate_rb, mate_fa, mate_fb):
        c.wait_send()
    for c in (halo, *d_far, *d_right, d_left_a, *d_left_b, d_own, *far_a, *far_b):
        c.wait_send()
    for c in (*r_a, *r_b, *l_a, *l_b):
        c.wait_send()
    for h in range(2):
        for what in range(3):
            exchange(h, 0, what).wait_send()
            exchange(h, 1, what).wait_send()
        for k in range(7):
            hand_out(h, k).wait_send()
    for chunk in range(2):
        for kind in range(2):
            for what in range(3):
                first_ring(chunk, kind, what).wait_send()
                for piece in range(4):
                    second_ring(chunk, kind, piece, what).wait_send()


def whole_layer(*args):
    vm = pl.BlockSpec(memory_space=pltpu.VMEM)
    sm = pl.BlockSpec(memory_space=pltpu.SMEM)
    hbm = pl.BlockSpec(memory_space=pl.ANY)
    block = [(128, WIDTH)] * 6
    return pl.pallas_call(
        layer_kernel,
        out_shape=jax.ShapeDtypeStruct((128, WIDTH), BF16),
        in_specs=[hbm] * 6 + [vm] * 3 + [sm] * 2 + [vm, hbm, vm, hbm, hbm, hbm, hbm, vm],
        out_specs=vm,
        scratch_shapes=[
            *[pltpu.VMEM((2 * NBLK, BLK), F32)] * 3,
            pltpu.VMEM((NBLK, 256, 128), BF16),
            pltpu.VMEM((NBLK, 192, 64), BF16),
            pltpu.VMEM((NBLK, BLK, BLK), F32),
            pltpu.VMEM((NBLK, BLK, BLK), F32),
            pltpu.VMEM((NBLK, 128, BLK), F32),
            pltpu.VMEM((NBLK, 64, BLK), F32),
            pltpu.VMEM((2048, BLK), F32),
            pltpu.VMEM((2048, BLK), F32),
            pltpu.VMEM((1024, 128), BF16),
            pltpu.VMEM((1024, 64), BF16),
            pltpu.VMEM((1024, BLK), F32),
            pltpu.VMEM((1024, BLK), F32),
            *[pltpu.VMEM((4, 272, 128), BF16), pltpu.VMEM((4, 128, 128), BF16)] * 2,
            pltpu.VMEM((2, 8, 128, 128), BF16),
            pltpu.VMEM((2, 8, 128, 128), BF16),
            pltpu.VMEM((WIDTH, WIDTH), BF16),
            pltpu.VMEM((128, WIDTH), F32),
            pltpu.VMEM((128, WIDTH), BF16),
            pltpu.VMEM((WIDTH, 2 * UNITS), BF16),
            pltpu.VMEM((16, UNITS, BLK), BF16),
            pltpu.VMEM((128, UNITS), BF16),
            *[pltpu.VMEM((1024, 128), BF16)] * 2,
            *[pltpu.VMEM((64, 1024), BF16)] * 2,
            *[pltpu.VMEM((2048, BLK), BF16)] * 2,
            pltpu.VMEM((128, WIDTH), BF16),
            pltpu.VMEM((1024, WIDTH), BF16),
            pltpu.VMEM((12, 1032, BLK), F32),
            pltpu.VMEM((1024, UNITS), BF16),
            pltpu.VMEM((4, 128, WIDTH), F32),
            pltpu.VMEM((4, 128, WIDTH), BF16),
            pltpu.VMEM((4, 128, WIDTH), BF16),
            *[pltpu.VMEM(b, BF16) for b in block],
            pltpu.SemaphoreType.DMA((11,)),
            pltpu.SemaphoreType.DMA((61,)),
            pltpu.SemaphoreType.DMA((61,)),
            pltpu.SemaphoreType.DMA((60,)),
            pltpu.SemaphoreType.DMA((60,)),
        ],
        compiler_params=pltpu.CompilerParams(
            collective_id=1, has_side_effects=True, vmem_limit_bytes=62 * 1024 * 1024
        ),
    )(*args)


def per_device(
    arriving_hidden_state,
    former_request_vectors,
    former_match_vectors,
    latter_request_vectors,
    latter_match_vectors,
    stored_vectors_both,
    closing_valve_operands,
    update_level_before_squash,
    fading_data_input,
    sparse_fading_boost,
    unitwise_fading_loglevel,
    fading_constant_term,
    unitwise_normalizer_coef,
    emission_map_weights,
    channel_normalizer_coef,
    switching_channel_map,
    broadening_channel_map,
    timewise_convolve_tapvalues,
    narrowing_map_weights_in,
):
    return whole_layer(
        former_request_vectors,
        former_match_vectors,
        latter_request_vectors.T,
        latter_match_vectors.T,
        stored_vectors_both.reshape(-1, 128),
        closing_valve_operands.reshape(-1, 128),
        update_level_before_squash.reshape(2, -1),
        fading_data_input,
        sparse_fading_boost,
        unitwise_fading_loglevel.reshape(1, 2),
        fading_constant_term.reshape(1, 2),
        unitwise_normalizer_coef.reshape(1, -1),
        emission_map_weights,
        channel_normalizer_coef.reshape(1, -1),
        arriving_hidden_state,
        switching_channel_map,
        broadening_channel_map,
        narrowing_map_weights_in,
        timewise_convolve_tapvalues,
    )


def solution(mesh):
    torus = Mesh(mesh.devices.reshape(4, 4, mesh.shape["tp"]), ("sp_0", "sp_1", "tp"))
    return jax.shard_map(
        per_device,
        mesh=torus,
        in_specs=(
            P(SP_TP, None),
            P(SP, "tp"),
            P(SP, "tp"),
            P(SP, "tp"),
            P(SP, "tp"),
            P(SP, None, "tp"),
            P(SP, None, "tp"),
            P(None, "tp", SP),
            P(None, "tp", SP),
            P(None, "tp", SP),
            P(None, "tp"),
            P(None, "tp"),
            P(),
            P(),
            P(),
            P(SP, "tp"),
            P(SP, "tp"),
            P(None, None, "tp"),
            P(SP, "tp"),
        ),
        out_specs=P(SP_TP, None),
        check_vma=False,
    )
```
